32 devices in a mesh: kv: 8 (over z, y), tp: 4 (over x, core).
Axes of the slice: x: 2, y: 2, z: 4, core: 2. Of those that a mesh axis runs over, the one named last changes fastest.
Arguments:
- tokens: bfloat16 [64, 4096], P(None, 'kv'), may hold values from -170 to 170
- mix_gain: float32 [4096], P('kv'), may hold values from 0.1 to 1.9
- w_query: bfloat16 [4096, 2048], P('kv', 'tp'), may hold values from -0.09375 to 0.09375
- w_key: bfloat16 [4096, 512], P('kv', 'tp'), may hold values from -0.09375 to 0.09375
- w_value: bfloat16 [4096, 512], P('kv', 'tp'), may hold values from -0.09375 to 0.09375
- w_forget: bfloat16 [4096, 32], P('kv', 'tp'), may hold values from -0.09375 to 0.09375
- query_gain: float32 [64], replicated, may hold values from 0.1 to 1.9
- key_cache: bfloat16 [64, 8, 64, 8192], P(None, 'tp', None, 'kv'), may hold values from -1300 to 1300
- value_cache: bfloat16 [64, 8, 64, 8192], P(None, 'tp', None, 'kv'), may hold values from -8 to 8
- decay_cache: float32 [64, 32, 8192], P(None, 'tp', 'kv'), may hold values from -1066.96 to 0, as said below
- w_out: bfloat16 [2048, 4096], P('tp', 'kv'), may hold values from -1 to 1
- mlp_gain: float32 [4096], P('kv'), may hold values from 0.1 to 1.9
- w_up: bfloat16 [4096, 16384], P('kv', 'tp'), may hold values from -0.09375 to 0.09375
- w_down: bfloat16 [16384, 4096], P('tp', 'kv'), may hold values from -0.046875 to 0.046875
Outputs:
- layer_out: bfloat16 [64, 4096], P(None, 'kv')
The draws below stay inside these ranges and needn't reach their ends.
Inputs may be any that keep to these rules, and one draw needn't show every extreme that they name: `decay_cache`: each entry is the sum of the non-positive log forget gates of the later cached positions of its sequence and head: 0 at the last cached position, never smaller at a later position.
All inputs are finite; a program needn't handle non-finite values.
Results may differ from the reference program's by a relative error of at most 0.015.
Values may be sent and summed in bfloat16 or wider, within the bound.
A program may use at most 128 MiB of HBM per device.

```python
import jax
import jax.numpy as jnp
from jax import lax

D = 4096
HEADS = 32
KV_HEADS = 8
HEAD_DIM = 64
FF = 16384
BATCH = 64
POSITIONS_LOCAL = 1024
POSITIONS = 8192
HEAD_GROUP = 8
FF_GROUP = 4096


def draw_tokens(key, part):
    keys = jax.random.split(key, 2)
    columns = jnp.arange(D, dtype=jnp.float32) / D
    base = jnp.clip(jax.random.normal(keys[0], (BATCH, D), jnp.float32), -4.0, 4.0)
    row_scale = jnp.exp(jax.random.uniform(keys[1], (BATCH, 1), jnp.float32, 0.0, jnp.log(3.0)))
    rising = 3.0 ** columns
    return (base * row_scale * rising[None, :]).astype(jnp.bfloat16)


def draw_key_cache(key, part):
    keys = jax.random.split(key, 3)
    base = jnp.clip(jax.random.normal(keys[0], (BATCH, KV_HEADS, HEAD_DIM, POSITIONS), jnp.float32), -5.0, 5.0)
    low_strength = jnp.log(40.0)
    high_strength = jnp.log(200.0)
    strength = jnp.exp(jax.random.uniform(keys[1], (BATCH, KV_HEADS, 1, 1), jnp.float32, low_strength, high_strength))
    spot = jax.random.randint(keys[2], (BATCH, KV_HEADS, 1, 1), 0, POSITIONS - 1)
    current_location = jnp.arange(POSITIONS).reshape(1, 1, 1, POSITIONS)
    anchor = jnp.take_along_axis(base, jnp.broadcast_to(spot, (BATCH, KV_HEADS, HEAD_DIM, 1)), axis=3)
    bump = jnp.where(current_location == spot + 1, 1.01, 1.0)
    planted = (current_location == spot) | (current_location == spot + 1)
    base = jnp.where(planted, anchor * strength * bump, base)
    return base.astype(jnp.bfloat16)


def draw_value_cache(key, part):
    keys = jax.random.split(key, 2)
    blocks = POSITIONS // POSITIONS_LOCAL
    base = jnp.clip(jax.random.normal(keys[0], (BATCH, KV_HEADS, HEAD_DIM, POSITIONS), jnp.float32), -5.0, 5.0)
    means = jnp.clip(jax.random.normal(keys[1], (BATCH, KV_HEADS, HEAD_DIM, blocks), jnp.float32), -3.0, 3.0)
    return (base + jnp.repeat(means, POSITIONS_LOCAL, axis=3)).astype(jnp.bfloat16)


def draw_decay_cache(key, part):
    keys = jax.random.split(key, 7)
    fast_share = 0.5
    is_fast = jax.random.uniform(keys[0], (BATCH, HEADS, 1), jnp.float32) < fast_share
    slow_rate = jax.random.uniform(keys[1], (BATCH, HEADS, 1), jnp.float32, 0.3, 0.8) / POSITIONS
    fast_rate = jnp.exp(jax.random.uniform(keys[2], (BATCH, HEADS, 1), jnp.float32, jnp.log(0.01), jnp.log(0.04)))
    baseline_rate = jnp.where(is_fast, fast_rate, slow_rate)
    blocks = POSITIONS // POSITIONS_LOCAL
    block_multiplier = jnp.exp(jax.random.uniform(keys[3], (BATCH, HEADS, blocks), jnp.float32, jnp.log(0.5), jnp.log(2.0)))
    coarse_estimate = jax.random.uniform(keys[4], (BATCH, HEADS, POSITIONS), jnp.float32, 0.5, 1.5)
    chosen_places = jax.random.randint(keys[5], (BATCH, HEADS, 2), 0, POSITIONS)
    loss_values = jax.random.uniform(keys[6], (BATCH, HEADS, 2), jnp.float32, 0.22, 0.69)
    current_location = jnp.arange(POSITIONS).reshape(1, 1, POSITIONS)
    sudden_jump = jnp.where(current_location == chosen_places[:, :, 0:1], loss_values[:, :, 0:1], 0.0)
    sudden_jump = sudden_jump + jnp.where(current_location == chosen_places[:, :, 1:2], loss_values[:, :, 1:2], 0.0)
    per_step_rate = baseline_rate * jnp.repeat(block_multiplier, POSITIONS_LOCAL, axis=2) * coarse_estimate + sudden_jump
    after = jnp.flip(jnp.cumsum(jnp.flip(per_step_rate, axis=2), axis=2), axis=2) - per_step_rate
    return -after


def shard_levels(key, extent, cuts, low, high):
    def one(axis_at, blocks):
        draws = jax.random.uniform(jax.random.fold_in(jax.random.fold_in(key, 6), axis_at), (blocks,), jnp.float32, low / len(cuts), high / len(cuts))
        return jnp.repeat(jnp.exp(draws), extent[axis_at] // blocks).reshape((-1,) + (1,) * (len(extent) - axis_at - 1))

    level = one(*cuts[0])
    for cut in cuts[1:]:
        level = level * one(*cut)
    return level


def bell_draw(own_key, dims, scale, limit, shards=(), kind=jnp.bfloat16):
    entries = jax.random.normal(own_key, dims, jnp.float32) * scale
    if len(shards) > 0:
        entries = shard_levels(own_key, dims, shards, -0.22, 0.18) * entries
    return jnp.clip(entries, min=-limit, max=limit).astype(kind)


def setup_inputs(seed: int = 0) -> dict:
    arg_keys = jax.random.split(jax.random.key(seed), 15)
    return {
        "tokens": draw_tokens(jax.random.fold_in(arg_keys[14], 71), 0),
        "mix_gain": jnp.clip(1.0 + 0.18 * jax.random.normal(arg_keys[1], (D,), jnp.float32), 0.1, 1.9),
        "w_query": bell_draw(arg_keys[2], (D, HEADS * HEAD_DIM), D ** -0.5, 0.09375, ((0, 8), (1, 4))),
        "w_key": bell_draw(arg_keys[3], (D, KV_HEADS * HEAD_DIM), D ** -0.5, 0.09375, ((0, 8), (1, 4))),
        "w_value": bell_draw(arg_keys[4], (D, KV_HEADS * HEAD_DIM), D ** -0.5, 0.09375, ((0, 8), (1, 4))),
        "w_forget": bell_draw(arg_keys[5], (D, HEADS), D ** -0.5, 0.09375, ((0, 8), (1, 4))),
        "query_gain": jnp.clip(1.0 + 0.18 * jax.random.normal(arg_keys[6], (HEAD_DIM,), jnp.float32), 0.1, 1.9),
        "key_cache": draw_key_cache(jax.random.fold_in(arg_keys[14], 71), 0),
        "value_cache": draw_value_cache(jax.random.fold_in(arg_keys[14], 71), 0),
        "decay_cache": draw_decay_cache(jax.random.fold_in(arg_keys[14], 71), 0),
        "w_out": bell_draw(arg_keys[10], (HEADS * HEAD_DIM, D), (HEADS * HEAD_DIM // 64) ** -0.5, 1.0, ((0, 4), (1, 8))),
        "mlp_gain": jnp.clip(1.0 + 0.18 * jax.random.normal(arg_keys[11], (D,), jnp.float32), 0.1, 1.9),
        "w_up": bell_draw(arg_keys[12], (D, FF), D ** -0.5, 0.09375, ((0, 8), (1, 4))),
        "w_down": bell_draw(arg_keys[13], (FF, D), FF ** -0.5, 0.046875, ((0, 4), (1, 8))),
    }


EPS = 1e-06

def rounded(value):
    return lax.optimization_barrier(value.astype(jnp.bfloat16)).astype(jnp.float32)

def attend_one(operands):
    query_row, keys_row, values_row, decay_row, forget_row, key_row, value_row = operands
    score_scale = HEAD_DIM ** (-0.5)
    scores = jnp.einsum('gjd,gdp->gjp', query_row.astype(jnp.float32), keys_row.astype(jnp.float32)) * score_scale
    scores = scores + decay_row + forget_row[..., None]
    own_score = jnp.einsum('gjd,gd->gj', query_row.astype(jnp.float32), key_row.astype(jnp.float32)) * score_scale
    peak_score = jnp.maximum(lax.optimization_barrier(jnp.max(scores, axis=-1)), own_score)
    weights = jnp.exp(scores - peak_score[..., None])
    own_weight = jnp.exp(own_score - peak_score)
    totals = lax.optimization_barrier(jnp.sum(weights, axis=-1)) + own_weight
    summed = jnp.einsum('gjp,gdp->gjd', rounded(weights), values_row.astype(jnp.float32))
    summed = summed + rounded(own_weight)[..., None] * value_row.astype(jnp.float32)[:, None, :]
    return summed / totals[..., None]

def reference(tokens, mix_gain, w_query, w_key, w_value, w_forget, query_gain, key_cache, value_cache, decay_cache, w_out, mlp_gain, w_up, w_down):
    stream = tokens.astype(jnp.float32)
    scale_mix = lax.rsqrt(lax.optimization_barrier(jnp.mean(stream * stream, axis=1, keepdims=True)) + EPS)
    normed_mix = (stream * mix_gain.astype(jnp.float32)).astype(jnp.bfloat16)
    query_raw = scale_mix * jnp.dot(normed_mix, w_query, preferred_element_type=jnp.float32)
    key_raw = scale_mix * jnp.dot(normed_mix, w_key, preferred_element_type=jnp.float32)
    value_raw = scale_mix * jnp.dot(normed_mix, w_value, preferred_element_type=jnp.float32)
    forget_raw = scale_mix * jnp.dot(normed_mix, w_forget, preferred_element_type=jnp.float32)
    heads_raw = query_raw.reshape(BATCH, HEADS, HEAD_DIM)
    inverse = lax.rsqrt(lax.optimization_barrier(jnp.mean(heads_raw * heads_raw, axis=-1, keepdims=True)) + EPS)
    query = (heads_raw * inverse * query_gain.astype(jnp.float32)).astype(jnp.bfloat16)
    sharing = HEADS // KV_HEADS
    query = query.reshape(BATCH, KV_HEADS, sharing, HEAD_DIM)
    key_new = key_raw.reshape(BATCH, KV_HEADS, HEAD_DIM).astype(jnp.bfloat16)
    value_new = value_raw.reshape(BATCH, KV_HEADS, HEAD_DIM).astype(jnp.bfloat16)
    log_forget = jax.nn.log_sigmoid(forget_raw).reshape(BATCH, KV_HEADS, sharing)
    decay = decay_cache.reshape(BATCH, KV_HEADS, sharing, -1)
    head_output = lax.map(attend_one, (query, key_cache, value_cache, decay, log_forget, key_new, value_new))
    attended = head_output.reshape(BATCH, HEADS * HEAD_DIM).astype(jnp.bfloat16)
    group_count = HEADS // HEAD_GROUP
    head_width = HEAD_GROUP * HEAD_DIM
    partials = jnp.einsum('bgk,gkd->bgd', attended.reshape(BATCH, group_count, head_width).astype(jnp.float32), w_out.reshape(group_count, head_width, D).astype(jnp.float32))
    attn_out = lax.optimization_barrier(jnp.sum(rounded(partials), axis=1))
    residual = (stream + rounded(attn_out)).astype(jnp.bfloat16)
    residual_wide = residual.astype(jnp.float32)
    scale_mlp = lax.rsqrt(lax.optimization_barrier(jnp.mean(residual_wide * residual_wide, axis=1, keepdims=True)) + EPS)
    normed_mlp = (residual_wide * mlp_gain.astype(jnp.float32)).astype(jnp.bfloat16)
    up_proj = scale_mlp * jnp.dot(normed_mlp, w_up, preferred_element_type=jnp.float32)
    hidden = jnp.square(jax.nn.relu(up_proj)).astype(jnp.bfloat16)
    unit_groups = FF // FF_GROUP
    down_parts = jnp.einsum('bgk,gkd->bgd', hidden.reshape(BATCH, unit_groups, FF_GROUP).astype(jnp.float32), w_down.reshape(unit_groups, FF_GROUP, D).astype(jnp.float32))
    mlp_out = lax.optimization_barrier(jnp.sum(rounded(down_parts), axis=1))
    return (residual_wide + rounded(mlp_out)).astype(jnp.bfloat16)
```

```python
import functools

import jax
import jax.numpy as jnp
from jax import lax
from jax.experimental import pallas as pl
from jax.experimental.pallas import tpu as pltpu
from jax.sharding import PartitionSpec as P

MESH = pl.DeviceIdType.MESH
HEAD_DIM = 64
EPS = 1e-06
DEPTH = 256
F32 = jnp.float32
BF16 = jnp.bfloat16


def greet(n, t):
    kv, tp = lax.axis_index("kv"), lax.axis_index("tp")
    barrier = pltpu.get_barrier_semaphore()
    for i in range(1, n):
        pl.semaphore_signal(
            barrier, inc=1, device_id=(lax.rem(kv + i, n), tp), device_id_type=MESH
        )
    for i in range(1, t):
        pl.semaphore_signal(
            barrier, inc=1, device_id=(kv, lax.rem(tp + i, t)), device_id_type=MESH
        )
    pl.semaphore_wait(barrier, n + t - 2)


def remote(src, dst, send, recv, kv, tp):
    return pltpu.make_async_remote_copy(
        src_ref=src,
        dst_ref=dst,
        send_sem=send,
        recv_sem=recv,
        device_id=(kv, tp),
        device_id_type=MESH,
    )


def split(x):
    hi = x.astype(BF16).astype(F32)
    return hi, (x - hi).astype(BF16).astype(F32)


def layer_kernel(
    n, t, d, sharing,
    mgain, qgain, pgain, tok_hbm, wq_hbm, wk_hbm, wv_hbm, wf_hbm,
    k_hbm, v_hbm, d_hbm, wo_hbm, wu_hbm, wd_hbm, out,
    tok, wq, wk, wv, wf, kbuf, vbuf, dbuf, wo, wu, wd,
    partq, partx, gotq, gotx, qs, qall, own, msg, gotm, heads_s,
    att, allatt, full, tpa, tpb, upsend, upgot, upsend2, upgot2, keep, sqs, sqgot, hid,
    wsem, ksem, vsem, dsem, sem, tsem,
):
    kv, tp = lax.axis_index("kv"), lax.axis_index("tp")
    rows, dl = tok.shape
    rc = rows // n
    nq, nk, heads = wq.shape[1], wk.shape[1], wf.shape[0]
    gd = (heads // sharing) * HEAD_DIM
    lines = rc * heads
    pack = DEPTH // gd
    tile = pack * heads

    def local(src, dst, s):
        return pltpu.make_async_copy(src, dst, s)

    def block_of(i):
        return lax.rem(kv + i, n)

    first = [
        local(a, b, wsem.at[j])
        for j, (a, b) in enumerate(
            ((tok_hbm, tok), (wq_hbm, wq), (wk_hbm, wk), (wv_hbm, wv), (wf_hbm, wf))
        )
    ]
    for c in first:
        c.start()

    def cache_loads(i):
        b = block_of(i)
        at = pl.ds(pl.multiple_of(b * rc * gd, rc * gd), rc * gd)
        lt = pl.ds(pl.multiple_of(b * lines, lines), lines)
        return (
            local(k_hbm.at[at], kbuf.at[at], ksem.at[i]),
            local(d_hbm.at[lt], dbuf.at[lt], dsem.at[i]),
            local(v_hbm.at[at], vbuf.at[at], vsem.at[i]),
        )

    for i in list(range(1, n)) + [0]:
        for c in cache_loads(i):
            c.start()
    late = [
        local(a, b, wsem.at[5 + j])
        for j, (a, b) in enumerate(((wo_hbm, wo), (wu_hbm, wu), (wd_hbm, wd)))
    ]
    for c in late:
        c.start()
    greet(n, t)
    started = []

    def send(kind, i, src, dst, peer=None):
        if peer is None:
            peer = lax.rem(kv + i, n)
        c = remote(src(peer), dst, sem.at[2 * kind, i], sem.at[2 * kind + 1, i], peer, tp)
        c.start()
        started.append(c)
        return c

    for c in first:
        c.wait()
    stream = tok[...].astype(F32)
    squares = jnp.sum(stream * stream, axis=1, keepdims=True)
    normed = (stream * mgain[...]).astype(BF16)
    q = jnp.dot(normed, wq[...], preferred_element_type=F32)
    f = lax.dot_general(
        normed, wf[...], (((1,), (1,)), ((), ())), preferred_element_type=F32
    )
    for p in range(n):
        cut = slice(p * rc, (p + 1) * rc)
        partq[p, :, 0:nq] = q[cut]
        partq[p, :, nq : nq + 128] = jnp.broadcast_to(squares[cut], (rc, 128))
        partq[p, :, nq : nq + heads] = f[cut]
    qcopies = [send(0, i, lambda p: partq.at[p], gotq.at[i]) for i in range(1, n)]
    k = jnp.dot(normed, wk[...], preferred_element_type=F32)
    v = jnp.dot(normed, wv[...], preferred_element_type=F32)
    for p in range(n):
        cut = slice(p * rc, (p + 1) * rc)
        partx[p, :, 0:nk] = k[cut]
        partx[p, :, nk : 2 * nk] = v[cut]
    xcopies = [send(1, i, lambda p: partx.at[p], gotx.at[i]) for i in range(1, n)]

    total = partq[kv]
    for c in qcopies:
        c.wait_recv()
    for i in range(1, n):
        total = total + gotq[i]
    scale = lax.rsqrt(total[:, nq + 127 : nq + 128] / d + EPS)
    raw = total[:, 0:nq] * scale
    gate = total[:, nq : nq + heads] * scale
    forget = jnp.minimum(gate, 0.0) - jnp.log1p(jnp.exp(-jnp.abs(gate)))
    queries = []
    for h in range(heads):
        part = raw[:, h * HEAD_DIM : (h + 1) * HEAD_DIM]
        mean = jnp.sum(part * part, axis=1, keepdims=True) / HEAD_DIM
        part = (part * lax.rsqrt(mean + EPS) * qgain[...]).astype(BF16).astype(F32)
        queries.append(part)
        g = h // sharing
        pieces = [part if j == g else jnp.zeros_like(part) for j in range(heads // sharing)]
        wide = jnp.concatenate(pieces, axis=1) if len(pieces) > 1 else part
        qs[pl.ds(h, rc, stride=heads), :] = wide
    qall[kv] = qs[...].astype(BF16)
    gathers = [send(2, i, lambda p: qall.at[kv], qall.at[kv]) for i in range(1, n)]
    extra = partx[kv]
    for c in xcopies:
        c.wait_recv()
    for i in range(1, n):
        extra = extra + gotx[i]
    extra = (extra * scale).astype(BF16).astype(F32)
    for h in range(heads):
        g = h // sharing
        key = extra[:, g * HEAD_DIM : (g + 1) * HEAD_DIM]
        value = extra[:, nk + g * HEAD_DIM : nk + (g + 1) * HEAD_DIM]
        score = jnp.sum(queries[h] * key, axis=1, keepdims=True) * (HEAD_DIM**-0.5)
        own[pl.ds(h, rc, stride=heads), :] = jnp.concatenate(
            [
                value,
                jnp.broadcast_to(score, (rc, 32)),
                jnp.broadcast_to(forget[:, h : h + 1], (rc, 32)),
            ],
            axis=1,
        )

    line = lax.broadcasted_iota(jnp.int32, (tile, gd), 0) // heads
    slot = lax.broadcasted_iota(jnp.int32, (tile, HEAD_DIM), 0) // sharing
    lane = lax.broadcasted_iota(jnp.int32, (tile, HEAD_DIM), 1) // 16

    def attend(b):
        steps = lines // tile
        scores, sums, peaks, outs = [], [], [], []
        for s in range(steps):
            qt = qall[b, s * tile : (s + 1) * tile, :]
            left = jnp.concatenate(
                [jnp.where(line == j, qt, jnp.zeros_like(qt)) for j in range(pack)], axis=1
            )
            at = pl.ds(pl.multiple_of(b * rc * gd + s * DEPTH, DEPTH), DEPTH)
            lt = pl.ds(pl.multiple_of(b * lines + s * tile, tile), tile)
            scores.append(
                jnp.dot(left, kbuf[at, :], preferred_element_type=F32) * (HEAD_DIM**-0.5)
                + dbuf[lt, :]
            )
        weights = []
        for s in range(steps):
            hi, lo = split(jnp.max(scores[s], axis=1, keepdims=True))
            w = jnp.exp(scores[s] - (hi + lo))
            peaks.append((hi, lo))
            sums.append(split(jnp.sum(w, axis=1, keepdims=True)))
            weights.append(w.astype(BF16))
        for s in range(steps):
            at = pl.ds(pl.multiple_of(b * rc * gd + s * DEPTH, DEPTH), DEPTH)
            o = lax.dot_general(
                weights[s], vbuf[at, :], (((1,), (1,)), ((), ())), preferred_element_type=F32
            )
            picked = o[:, 0:HEAD_DIM]
            for g in range(1, DEPTH // HEAD_DIM):
                picked = jnp.where(slot == g, o[:, g * HEAD_DIM : (g + 1) * HEAD_DIM], picked)
            stats = jnp.where(
                lane == 0,
                peaks[s][0],
                jnp.where(lane == 1, peaks[s][1], jnp.where(lane == 2, sums[s][0], sums[s][1])),
            )
            msg[b, s * tile : (s + 1) * tile, :] = jnp.concatenate(
                [picked, stats], axis=1
            ).astype(BF16)

    def message(i):
        b = block_of(i)
        return remote(msg.at[b], gotm.at[i], sem.at[6, i], sem.at[7, i], b, tp)

    def step(i, carry):
        b = block_of(i)
        remote(
            qall.at[b], qall.at[b], sem.at[4, n - i], sem.at[5, n - i], b, tp
        ).wait_recv()
        for c in cache_loads(i):
            c.wait()
        attend(b)
        message(i).start()
        return carry

    lax.fori_loop(1, n, step, 0)
    for c in cache_loads(0):
        c.wait()
    attend(kv)

    extra = own[...]
    own_score = extra[:, 64:65]
    forget = extra[:, 96:97]
    for i in range(1, n):
        message(i).wait_recv()
    blocks = [msg[kv].astype(F32)] + [gotm[i].astype(F32) for i in range(1, n)]
    peaks = [b[:, 64:65] + b[:, 80:81] + forget for b in blocks]
    peak = own_score
    for p in peaks:
        peak = jnp.maximum(peak, p)
    own_weight = jnp.exp(own_score - peak)
    mass = own_weight
    summed = own_weight.astype(BF16).astype(F32) * extra[:, 0:64]
    for b, p in zip(blocks, peaks):
        w = jnp.exp(p - peak)
        mass = mass + w * (b[:, 96:97] + b[:, 112:113])
        summed = summed + w * b[:, 0:64]
    heads_s[...] = summed / mass
    for h in range(0, heads, 2):
        att[:, h * HEAD_DIM : (h + 2) * HEAD_DIM] = jnp.concatenate(
            [
                heads_s[pl.ds(h, rc, stride=heads), :],
                heads_s[pl.ds(h + 1, rc, stride=heads), :],
            ],
            axis=1,
        ).astype(BF16)

    def tp_sum(kind, buf, value):
        buf[tp] = value.astype(BF16)
        copies = []
        for i in range(1, t):
            c = remote(
                buf.at[tp], buf.at[tp], tsem.at[2 * kind, i], tsem.at[2 * kind + 1, i],
                kv, lax.rem(tp + i, t),
            )
            c.start()
            copies.append(c)
            started.append(c)
        for c in copies:
            c.wait_recv()
        total = buf[0].astype(F32)
        for j in range(1, t):
            total = total + buf[j].astype(F32)
        return total.astype(BF16).astype(F32)

    ffc = wu.shape[1] // n
    copies = [send(4, i, lambda p: att, allatt.at[kv]) for i in range(1, n)]
    allatt[kv] = att[...]
    late[0].wait()
    for c in copies:
        c.wait_recv()
    for p in range(n):
        full[p * rc : (p + 1) * rc, :] = allatt[p].astype(F32)
    attn = jnp.dot(full[...].astype(BF16), wo[...], preferred_element_type=F32)
    attn = tp_sum(0, tpa, attn)
    residual = (tok[...].astype(F32) + attn).astype(BF16).astype(F32)
    normed = (residual * pgain[...]).astype(BF16)
    late[1].wait()
    half = n // 2
    side = lax.rem(kv, 2)
    place = kv // 2
    partner = kv + 1 - 2 * side
    order = list(range(1, half)) + [0]

    def term(dest):
        cols = pl.ds(pl.multiple_of(dest * ffc, ffc), ffc)
        return jnp.dot(normed, wu[:, cols], preferred_element_type=F32)

    firsts = {}
    for j in order:
        upsend[j] = term(2 * lax.rem(place + j, half) + 1 - side).astype(BF16)
        firsts[j] = send(5, j, lambda p: upsend.at[j], upgot.at[j], partner)
    for j in order:
        keep[j] = term(2 * lax.rem(place + j, half) + side)
    sqs[...] = lax.dot_general(
        jnp.ones((8, residual.shape[1]), F32),
        residual * residual,
        (((1,), (1,)), ((), ())),
        preferred_element_type=F32,
        precision=lax.Precision.HIGHEST,
    )
    sq_copies = [send(6, i, lambda p: sqs, sqgot.at[i]) for i in range(1, n)]
    seconds = {}
    for j in order:
        firsts[j].wait_recv()
        part = keep[j] + upgot[j].astype(F32)
        if j:
            upsend2[j] = part.astype(BF16)
            seconds[j] = send(
                7, j, lambda p: upsend2.at[j], upgot2.at[j], 2 * lax.rem(place + j, half) + side
            )
    total = sqs[...]
    for i in range(1, n):
        sq_copies[i - 1].wait_recv()
        total = total + sqgot[i]
    r = lax.broadcasted_iota(jnp.int32, (rows, rows), 0)
    c_ = lax.broadcasted_iota(jnp.int32, (rows, rows), 1)
    wide = jnp.broadcast_to(total[0:1, :], (rows, rows))
    column = jnp.sum(jnp.where(r == c_, wide, 0.0), axis=1, keepdims=True)
    scale = lax.rsqrt(column / d + EPS)
    for j in range(1, half):
        seconds[j].wait_recv()
        part = part + upgot2[j].astype(F32)
    hidden = jnp.square(jnp.maximum(part * scale, 0.0)).astype(BF16)
    hid[kv] = hidden
    across = {0: send(9, 0, lambda p: hid.at[kv], hid.at[kv], partner)}
    along = {}
    for j in range(1, half):
        along[j] = send(
            8, j, lambda p: hid.at[kv], hid.at[kv], 2 * lax.rem(place + j, half) + side
        )
    late[2].wait()

    def lower(src):
        there = pl.ds(pl.multiple_of(src * ffc, ffc), ffc)
        return jnp.dot(hid[src], wd[there, :], preferred_element_type=F32)

    down = lower(kv)
    for j in range(1, half):
        src = 2 * lax.rem(place + half - j, half) + side
        along[j].wait_recv()
        across[j] = send(9, j, lambda p: hid.at[src], hid.at[src], partner)
        down = down + lower(src)
    for j in range(half):
        across[j].wait_recv()
        down = down + lower(2 * lax.rem(place + half - j, half) + 1 - side)
    mlp = tp_sum(1, tpb, down)
    out[...] = (residual + mlp).astype(BF16)
    for i in range(1, n):
        message(i).wait_send()
    for c in started:
        c.wait_send()


def shards(
    n, t, tokens, mix_gain, w_query, w_key, w_value, w_forget, query_gain,
    key_cache, value_cache, decay_cache, w_out, mlp_gain, w_up, w_down,
):
    rows, dl = tokens.shape
    d = dl * n
    rc = rows // n
    heads = w_forget.shape[1]
    groups = key_cache.shape[1]
    sharing = heads // groups
    nq, nk = w_query.shape[1], w_key.shape[1]
    span = key_cache.shape[3]
    gd = groups * HEAD_DIM
    ffc = w_up.shape[1] // n
    half = n // 2
    vmem = pl.BlockSpec(memory_space=pltpu.VMEM)
    anywhere = pl.BlockSpec(memory_space=pl.ANY)
    dma = pltpu.SemaphoreType.DMA
    return pl.pallas_call(
        functools.partial(layer_kernel, n, t, d, sharing),
        out_shape=jax.ShapeDtypeStruct((rows, dl), BF16),
        in_specs=[vmem] * 3 + [anywhere] * 11,
        out_specs=vmem,
        scratch_shapes=[
            pltpu.VMEM(tokens.shape, BF16),
            pltpu.VMEM(w_query.shape, BF16),
            pltpu.VMEM(w_key.shape, BF16),
            pltpu.VMEM(w_value.shape, BF16),
            pltpu.VMEM((heads, dl), BF16),
            pltpu.VMEM((rows * gd, span), BF16),
            pltpu.VMEM((rows * gd, span), BF16),
            pltpu.VMEM((rows * heads, span), F32),
            pltpu.VMEM(w_out.shape, BF16),
            pltpu.VMEM(w_up.shape, BF16),
            pltpu.VMEM(w_down.shape, BF16),
            pltpu.VMEM((n, rc, nq + 128), F32),
            pltpu.VMEM((n, rc, 2 * nk), F32),
            pltpu.VMEM((n, rc, nq + 128), F32),
            pltpu.VMEM((n, rc, 2 * nk), F32),
            pltpu.VMEM((rc * heads, gd), F32),
            pltpu.VMEM((n, rc * heads, gd), BF16),
            pltpu.VMEM((rc * heads, 128), F32),
            pltpu.VMEM((n, rc * heads, 128), BF16),
            pltpu.VMEM((n, rc * heads, 128), BF16),
            pltpu.VMEM((rc * heads, HEAD_DIM), F32),
            pltpu.VMEM((rc, nq), BF16),
            pltpu.VMEM((n, rc, nq), BF16),
            pltpu.VMEM((rows, nq), F32),
            pltpu.VMEM((t, rows, dl), BF16),
            pltpu.VMEM((t, rows, dl), BF16),
            pltpu.VMEM((half, rows, ffc), BF16),
            pltpu.VMEM((half, rows, ffc), BF16),
            pltpu.VMEM((half, rows, ffc), BF16),
            pltpu.VMEM((half, rows, ffc), BF16),
            pltpu.VMEM((half, rows, ffc), F32),
            pltpu.VMEM((8, rows), F32),
            pltpu.VMEM((n, 8, rows), F32),
            pltpu.VMEM((n, rows, ffc), BF16),
            dma((8,)), dma((n,)), dma((n,)), dma((n,)), dma((20, n)), dma((4, t)),
        ],
        compiler_params=pltpu.CompilerParams(
            collective_id=0, has_side_effects=True, vmem_limit_bytes=60 * 2**20
        ),
    )(
        mix_gain[None, :], query_gain[None, :], mlp_gain[None, :],
        tokens, w_query, w_key, w_value, w_forget.T,
        key_cache.reshape(rows * gd, span),
        value_cache.reshape(rows * gd, span),
        decay_cache.reshape(rows * heads, span),
        w_out, w_up, w_down,
    )


def solution(mesh):
    in_specs = (
        P(None, "kv"),
        P("kv"),
        P("kv", "tp"),
        P("kv", "tp"),
        P("kv", "tp"),
        P("kv", "tp"),
        P(),
        P(None, "tp", None, "kv"),
        P(None, "tp", None, "kv"),
        P(None, "tp", "kv"),
        P("tp", "kv"),
        P("kv"),
        P("kv", "tp"),
        P("tp", "kv"),
    )
    body = functools.partial(shards, mesh.shape["kv"], mesh.shape["tp"])
    return jax.shard_map(
        body, mesh=mesh, in_specs=in_specs, out_specs=P(None, "kv"), check_vma=False
    )
```

```python
import functools

import jax
import jax.numpy as jnp
from jax import lax
from jax.experimental import pallas as pl
from jax.experimental.pallas import tpu as pltpu
from jax.sharding import PartitionSpec as P

MESH = pl.DeviceIdType.MESH
HEAD_DIM = 64
EPS = 1e-06
DEPTH = 256
F32 = jnp.float32
BF16 = jnp.bfloat16


def greet(n, t):
    kv, tp = lax.axis_index("kv"), lax.axis_index("tp")
    barrier = pltpu.get_barrier_semaphore()
    for i in range(1, n):
        pl.semaphore_signal(
            barrier, inc=1, device_id=(lax.rem(kv + i, n), tp), device_id_type=MESH
        )
    for i in range(1, t):
        pl.semaphore_signal(
            barrier, inc=1, device_id=(kv, lax.rem(tp + i, t)), device_id_type=MESH
        )
    pl.semaphore_wait(barrier, n + t - 2)


def remote(src, dst, send, recv, kv, tp):
    return pltpu.make_async_remote_copy(
        src_ref=src,
        dst_ref=dst,
        send_sem=send,
        recv_sem=recv,
        device_id=(kv, tp),
        device_id_type=MESH,
    )


def semaphores(n, parts):
    half = n // 2
    sizes = dict(
        first=5, late=3, cache=3 * parts, q=2, x=2, g=2, m=1 + parts, a=1 + parts,
        t0=1 + parts, t1=1 + parts, y=1 + parts * half, s=1 + parts, z=1 + parts,
        along=1 + parts * half, across=1 + parts * half,
    )
    at, total = {}, 0
    for name, size in sizes.items():
        at[name] = total
        total += size
    return at, total


def split(x):
    hi = x.astype(BF16).astype(F32)
    return hi, (x - hi).astype(BF16).astype(F32)


def layer_kernel(
    n, t, d, sharing, parts,
    mgain, qgain, pgain, tok_hbm, wq_hbm, wk_hbm, wv_hbm, wf_hbm,
    k_hbm, v_hbm, d_hbm, wo_hbm, wu_hbm, wd_hbm, out,
    tok, wq, wk, wv, wf, kbuf, vbuf, dbuf, wo, wu, wd,
    partq, partx, gotq, gotx, qs, qall, own, msg, gotm, heads_s,
    att, allatt, full, tpa, tpb, upsend, upgot, upsend2, upgot2, keep, sqs, sqgot, hid,
    sem,
):
    kv, tp = lax.axis_index("kv"), lax.axis_index("tp")
    rows, dl = tok.shape
    rc = rows // n
    rh = rows // parts
    rb = rh // n
    nq, nk, heads = wq.shape[1], wk.shape[1], wf.shape[0]
    groups = heads // sharing
    gd = groups * HEAD_DIM
    lines = rb * heads
    pack = DEPTH // gd
    tile = pack * heads
    ffc = wu.shape[1] // n

    at_sem, _ = semaphores(n, parts)

    def flag(name, i=0):
        return sem.at[at_sem[name] + i]

    def local(src, dst, s):
        return pltpu.make_async_copy(src, dst, s)

    def drain(ref, s):
        pltpu.make_async_copy(ref, ref, s).wait()

    def block_of(i):
        return lax.rem(kv + i, n)

    first = [
        local(a, b, flag("first", j))
        for j, (a, b) in enumerate(
            ((tok_hbm, tok), (wq_hbm, wq), (wk_hbm, wk), (wv_hbm, wv), (wf_hbm, wf))
        )
    ]
    for c in first:
        c.start()

    def cache_loads(h):
        at = pl.ds(h * rh * gd, rh * gd)
        lt = pl.ds(h * rh * heads, rh * heads)
        return (
            local(k_hbm.at[at], kbuf.at[at], flag("cache", 3 * h)),
            local(d_hbm.at[lt], dbuf.at[lt], flag("cache", 3 * h + 1)),
            local(v_hbm.at[at], vbuf.at[at], flag("cache", 3 * h + 2)),
        )

    for h in range(parts):
        for c in cache_loads(h):
            c.start()
    late = [
        local(a, b, flag("late", j))
        for j, (a, b) in enumerate(((wo_hbm, wo), (wu_hbm, wu), (wd_hbm, wd)))
    ]
    for c in late:
        c.start()
    greet(n, t)

    def send(name, src, dst, peer, slot=0):
        remote(src, dst, flag(name), flag(name, 1 + slot), peer, tp).start()

    def to_all(name, src, dst, slot=0):
        for i in range(1, n):
            peer = lax.rem(kv + i, n)
            send(name, src(peer), dst(i), peer, slot)

    for c in first:
        c.wait()
    stream = tok[...].astype(F32)
    squares = jnp.sum(stream * stream, axis=1, keepdims=True)
    normed = (stream * mgain[...]).astype(BF16)
    q = jnp.dot(normed, wq[...], preferred_element_type=F32)
    f = lax.dot_general(
        normed, wf[...], (((1,), (1,)), ((), ())), preferred_element_type=F32
    )
    pieces = [
        (p, slice(h * rb, (h + 1) * rb), slice(h * rh + p * rb, h * rh + (p + 1) * rb))
        for p in range(n)
        for h in range(parts)
    ]
    for p, to, cut in pieces:
        partq[p, to, 0:nq] = q[cut]
        partq[p, to, nq : nq + 128] = jnp.broadcast_to(squares[cut], (rb, 128))
        partq[p, to, nq : nq + heads] = f[cut]
    to_all("q", lambda p: partq.at[p], lambda i: gotq.at[i])
    k = jnp.dot(normed, wk[...], preferred_element_type=F32)
    v = jnp.dot(normed, wv[...], preferred_element_type=F32)
    for p, to, cut in pieces:
        partx[p, to, 0:nk] = k[cut]
        partx[p, to, nk : 2 * nk] = v[cut]
    to_all("x", lambda p: partx.at[p], lambda i: gotx.at[i])

    total = partq[kv]
    others = pl.ds(1, n - 1)
    drain(gotq.at[others], flag("q", 1))
    for i in range(1, n):
        total = total + gotq[i]
    scale = lax.rsqrt(total[:, nq + 127 : nq + 128] / d + EPS)
    raw = total[:, 0:nq] * scale
    gate = total[:, nq : nq + heads] * scale
    forget = jnp.minimum(gate, 0.0) - jnp.log1p(jnp.exp(-jnp.abs(gate)))
    queries = []
    for h in range(heads):
        part = raw[:, h * HEAD_DIM : (h + 1) * HEAD_DIM]
        mean = jnp.sum(part * part, axis=1, keepdims=True) / HEAD_DIM
        part = (part * lax.rsqrt(mean + EPS) * qgain[...]).astype(BF16).astype(F32)
        queries.append(part)
    for j in range(sharing):
        side_by_side = [queries[g * sharing + j] for g in range(groups)]
        qs[pl.ds(j, rc, stride=sharing), :] = (
            jnp.concatenate(side_by_side, axis=1) if groups > 1 else side_by_side[0]
        )
    for h in range(parts):
        qall[kv, h] = qs[h * rb * sharing : (h + 1) * rb * sharing, :].astype(BF16)
    to_all("g", lambda p: qall.at[kv], lambda i: qall.at[kv])
    extra = partx[kv]
    drain(gotx.at[others], flag("x", 1))
    for i in range(1, n):
        extra = extra + gotx[i]
    extra = (extra * scale).astype(BF16).astype(F32)
    for h in range(heads):
        g = h // sharing
        key = extra[:, g * HEAD_DIM : (g + 1) * HEAD_DIM]
        value = extra[:, nk + g * HEAD_DIM : nk + (g + 1) * HEAD_DIM]
        score = jnp.sum(queries[h] * key, axis=1, keepdims=True) * (HEAD_DIM**-0.5)
        own[pl.ds(h, rc, stride=heads), :] = jnp.concatenate(
            [
                value,
                jnp.broadcast_to(score, (rc, 32)),
                jnp.broadcast_to(forget[:, h : h + 1], (rc, 32)),
            ],
            axis=1,
        )

    group_row = lax.broadcasted_iota(jnp.int32, (heads, gd), 0) // sharing
    group_lane = lax.broadcasted_iota(jnp.int32, (heads, gd), 1) // HEAD_DIM
    slot = lax.broadcasted_iota(jnp.int32, (tile, HEAD_DIM), 0) // sharing
    lane = lax.broadcasted_iota(jnp.int32, (tile, HEAD_DIM), 1) // 16

    def attend(h, bs):
        todo = [(b, s) for b in bs for s in range(lines // tile)]
        scores, sums, peaks = [], [], []
        for b, s in todo:
            qt = qall[b, h].astype(F32)
            strips = []
            for j in range(pack):
                at = (s * pack + j) * sharing
                one = jnp.concatenate([qt[at : at + sharing]] * groups, axis=0)
                one = jnp.where(group_row == group_lane, one, 0.0)
                zero = jnp.zeros_like(one)
                strips.append(
                    jnp.concatenate([one if m == j else zero for m in range(pack)], axis=1)
                )
            left = jnp.concatenate(strips, axis=0).astype(BF16)
            row = h * rh + b * rb + s * pack
            at = pl.ds(pl.multiple_of(row * gd, DEPTH), DEPTH)
            lt = pl.ds(pl.multiple_of(row * heads, tile), tile)
            scores.append(
                jnp.dot(left, kbuf[at, :], preferred_element_type=F32) * (HEAD_DIM**-0.5)
                + dbuf[lt, :]
            )
        weights = []
        for sc in scores:
            hi, lo = split(jnp.max(sc, axis=1, keepdims=True))
            w = jnp.exp(sc - (hi + lo))
            peaks.append((hi, lo))
            sums.append(split(jnp.sum(w, axis=1, keepdims=True)))
            weights.append(w.astype(BF16))
        for (b, s), w, top, mass in zip(todo, weights, peaks, sums):
            row = h * rh + b * rb + s * pack
            at = pl.ds(pl.multiple_of(row * gd, DEPTH), DEPTH)
            o = lax.dot_general(
                w, vbuf[at, :], (((1,), (1,)), ((), ())), preferred_element_type=F32
            )
            picked = o[:, 0:HEAD_DIM]
            for g in range(1, DEPTH // HEAD_DIM):
                picked = jnp.where(slot == g, o[:, g * HEAD_DIM : (g + 1) * HEAD_DIM], picked)
            stats = jnp.where(
                lane == 0,
                top[0],
                jnp.where(lane == 1, top[1], jnp.where(lane == 2, mass[0], mass[1])),
            )
            msg[h, b, s * tile : (s + 1) * tile, :] = jnp.concatenate(
                [picked, stats], axis=1
            ).astype(BF16)

    twin = n // 2

    def step(u, h):
        i0 = 1 + 2 * u
        i1 = lax.rem(i0 + 1, n)
        attend(h, [block_of(i0), block_of(i1)])

        def message(i):
            b = block_of(i)
            send("m", msg.at[h, b], gotm.at[h, i], b, h)

        message(i0)

        @pl.when(i1 != 0)
        def _():
            message(i1)

        return h

    def attend_half(h, start, stop):
        lax.fori_loop(start, stop, lambda u, carry: step(u, h) * 0, 0)

    def combine(h):
        extra = own[h * lines : (h + 1) * lines, :]
        own_score = extra[:, 64:65]
        forget = extra[:, 96:97]
        drain(gotm.at[h, others], flag("m", 1 + h))
        blocks = [msg[h, kv].astype(F32)] + [gotm[h, i].astype(F32) for i in range(1, n)]
        peaks = [b[:, 64:65] + b[:, 80:81] + forget for b in blocks]
        peak = own_score
        for p in peaks:
            peak = jnp.maximum(peak, p)
        own_weight = jnp.exp(own_score - peak)
        mass = own_weight
        summed = own_weight.astype(BF16).astype(F32) * extra[:, 0:64]
        for b, p in zip(blocks, peaks):
            w = jnp.exp(p - peak)
            mass = mass + w * (b[:, 96:97] + b[:, 112:113])
            summed = summed + w * b[:, 0:64]
        heads_s[h] = summed / mass
        for j in range(0, heads, 2):
            pair = [heads_s[h, pl.ds(j + m, rb, stride=heads), :] for m in range(2)]
            att[h, :, j * HEAD_DIM : (j + 2) * HEAD_DIM] = jnp.concatenate(
                pair, axis=1
            ).astype(BF16)
        allatt[h, kv] = att[h]
        to_all("a", lambda p: att.at[h], lambda i: allatt.at[h, kv], h)

    def tp_send(name, h, buf, value):
        buf[h, tp] = value.astype(BF16)
        for i in range(1, t):
            remote(
                buf.at[h, tp], buf.at[h, tp], flag(name), flag(name, 1 + h),
                kv, lax.rem(tp + i, t),
            ).start()

    def tp_total(name, h, buf):
        drain(buf.at[h, pl.ds(1, t - 1)], flag(name, 1 + h))
        total = buf[h, 0].astype(F32)
        for j in range(1, t):
            total = total + buf[h, j].astype(F32)
        return total.astype(BF16).astype(F32)

    def project_out(h):
        drain(allatt.at[h, others], flag("a", 1 + h))
        for p in range(n):
            full[h, p * rb : (p + 1) * rb, :] = allatt[h, p].astype(F32)
        attn = jnp.dot(full[h].astype(BF16), wo[...], preferred_element_type=F32)
        tp_send("t0", h, tpa, attn)

    half = n // 2
    side = lax.rem(kv, 2)
    place = kv // 2
    partner = kv + 1 - 2 * side
    order = list(range(1, half)) + [0]

    def up_start(h):
        attn = tp_total("t0", h, tpa)
        residual = (tok[h * rh : (h + 1) * rh, :].astype(F32) + attn).astype(BF16).astype(F32)
        normed = (residual * pgain[...]).astype(BF16)

        def term(dest):
            cols = pl.ds(pl.multiple_of(dest * ffc, ffc), ffc)
            return jnp.dot(normed, wu[:, cols], preferred_element_type=F32)

        for j in order:
            upsend[h, j] = term(2 * lax.rem(place + j, half) + 1 - side).astype(BF16)
            send("y", upsend.at[h, j], upgot.at[h, j], partner, h * half + j)
        for j in order:
            keep[h, j] = term(2 * lax.rem(place + j, half) + side)
        sqs[h] = lax.dot_general(
            jnp.ones((8, dl), F32),
            residual * residual,
            (((1,), (1,)), ((), ())),
            preferred_element_type=F32,
            precision=lax.Precision.HIGHEST,
        )
        to_all("s", lambda p: sqs.at[h], lambda i: sqgot.at[h, i], h)
        return residual

    def up_middle(h):
        for j in order:
            drain(upgot.at[h, j], flag("y", 1 + h * half + j))
            part = keep[h, j] + upgot[h, j].astype(F32)
            if j:
                upsend2[h, j] = part.astype(BF16)
                send(
                    "z", upsend2.at[h, j], upgot2.at[h, j],
                    2 * lax.rem(place + j, half) + side, h,
                )
        return part

    def up_finish(h, part):
        drain(sqgot.at[h, others], flag("s", 1 + h))
        total = sqs[h]
        for i in range(1, n):
            total = total + sqgot[h, i]
        r = lax.broadcasted_iota(jnp.int32, (rh, rh), 0)
        c_ = lax.broadcasted_iota(jnp.int32, (rh, rh), 1)
        wide = jnp.broadcast_to(total[0:1, :], (rh, rh))
        column = jnp.sum(jnp.where(r == c_, wide, 0.0), axis=1, keepdims=True)
        scale = lax.rsqrt(column / d + EPS)
        drain(upgot2.at[h, pl.ds(1, half - 1)], flag("z", 1 + h))
        for j in range(1, half):
            part = part + upgot2[h, j].astype(F32)
        hid[h, kv] = jnp.square(jnp.maximum(part * scale, 0.0)).astype(BF16)
        mine = hid.at[h, kv]
        send("across", mine, mine, partner, h * half)
        for j in range(1, half):
            send("along", mine, mine, 2 * lax.rem(place + j, half) + side, h * half + j)

    def lower(h, src):
        there = pl.ds(pl.multiple_of(src * ffc, ffc), ffc)
        return jnp.dot(hid[h, src], wd[there, :], preferred_element_type=F32)

    def down_start(h):
        down = lower(h, kv)
        for j in range(1, half):
            src = 2 * lax.rem(place + half - j, half) + side
            block = hid.at[h, src]
            drain(block, flag("along", 1 + h * half + j))
            send("across", block, block, partner, h * half + j)
            down = down + lower(h, src)
        return down

    def down_finish(h, down):
        for j in range(half):
            src = 2 * lax.rem(place + half - j, half) + 1 - side
            drain(hid.at[h, src], flag("across", 1 + h * half + j))
            down = down + lower(h, src)
        tp_send("t1", h, tpb, down)

    each = range(parts)
    last = parts - 1
    drain(qall.at[others], flag("g", 1))
    for h in each:
        for c in cache_loads(h):
            c.wait()
        if h < last or parts == 1:
            attend_half(h, 0, twin)
        else:
            attend_half(h, 0, twin // 2)
            for e in range(last):
                combine(e)
            attend_half(h, twin // 2, twin)
    combine(last)
    late[0].wait()
    for h in each:
        project_out(h)
    late[1].wait()
    residuals = {h: up_start(h) for h in each}
    mids = {h: up_middle(h) for h in each}
    for h in each:
        up_finish(h, mids[h])
    late[2].wait()
    downs = {h: down_start(h) for h in each}
    for h in each:
        down_finish(h, downs[h])
    for h in each:
        out[h * rh : (h + 1) * rh, :] = (residuals[h] + tp_total("t1", h, tpb)).astype(BF16)
    rest = pl.ds(1, half - 1)
    drain(gotq.at[others], flag("q"))
    drain(gotx.at[others], flag("x"))
    drain(qall.at[others], flag("g"))
    drain(gotm.at[:, others], flag("m"))
    drain(allatt.at[:, others], flag("a"))
    drain(tpa.at[:, pl.ds(1, t - 1)], flag("t0"))
    drain(upsend, flag("y"))
    drain(sqgot.at[:, others], flag("s"))
    drain(upgot2.at[:, rest], flag("z"))
    drain(upgot2.at[:, rest], flag("along"))
    drain(upgot, flag("across"))
    drain(tpb.at[:, pl.ds(1, t - 1)], flag("t1"))


def shards(
    n, t, tokens, mix_gain, w_query, w_key, w_value, w_forget, query_gain,
    key_cache, value_cache, decay_cache, w_out, mlp_gain, w_up, w_down,
):
    rows, dl = tokens.shape
    d = dl * n
    rc = rows // n
    heads = w_forget.shape[1]
    groups = key_cache.shape[1]
    sharing = heads // groups
    nq, nk = w_query.shape[1], w_key.shape[1]
    span = key_cache.shape[3]
    gd = groups * HEAD_DIM
    ffc = w_up.shape[1] // n
    half = n // 2
    parts = 2 if (rows // n) % (2 * (DEPTH // gd)) == 0 else 1
    rh = rows // parts
    rb = rh // n
    lines = rb * heads
    vmem = pl.BlockSpec(memory_space=pltpu.VMEM)
    anywhere = pl.BlockSpec(memory_space=pl.ANY)
    dma = pltpu.SemaphoreType.DMA
    return pl.pallas_call(
        functools.partial(layer_kernel, n, t, d, sharing, parts),
        out_shape=jax.ShapeDtypeStruct((rows, dl), BF16),
        in_specs=[vmem] * 3 + [anywhere] * 11,
        out_specs=vmem,
        scratch_shapes=[
            pltpu.VMEM(tokens.shape, BF16),
            pltpu.VMEM(w_query.shape, BF16),
            pltpu.VMEM(w_key.shape, BF16),
            pltpu.VMEM(w_value.shape, BF16),
            pltpu.VMEM((heads, dl), BF16),
            pltpu.VMEM((rows * gd, span), BF16),
            pltpu.VMEM((rows * gd, span), BF16),
            pltpu.VMEM((rows * heads, span), F32),
            pltpu.VMEM(w_out.shape, BF16),
            pltpu.VMEM(w_up.shape, BF16),
            pltpu.VMEM(w_down.shape, BF16),
            pltpu.VMEM((n, rc, nq + 128), F32),
            pltpu.VMEM((n, rc, 2 * nk), F32),
            pltpu.VMEM((n, rc, nq + 128), F32),
            pltpu.VMEM((n, rc, 2 * nk), F32),
            pltpu.VMEM((rc * sharing, gd), F32),
            pltpu.VMEM((n, parts, rb * sharing, gd), BF16),
            pltpu.VMEM((rc * heads, 128), F32),
            pltpu.VMEM((parts, n, lines, 128), BF16),
            pltpu.VMEM((parts, n, lines, 128), BF16),
            pltpu.VMEM((parts, lines, HEAD_DIM), F32),
            pltpu.VMEM((parts, rb, nq), BF16),
            pltpu.VMEM((parts, n, rb, nq), BF16),
            pltpu.VMEM((parts, rh, nq), F32),
            pltpu.VMEM((parts, t, rh, dl), BF16),
            pltpu.VMEM((parts, t, rh, dl), BF16),
            pltpu.VMEM((parts, half, rh, ffc), BF16),
            pltpu.VMEM((parts, half, rh, ffc), BF16),
            pltpu.VMEM((parts, half, rh, ffc), BF16),
            pltpu.VMEM((parts, half, rh, ffc), BF16),
            pltpu.VMEM((parts, half, rh, ffc), F32),
            pltpu.VMEM((parts, 8, rh), F32),
            pltpu.VMEM((parts, n, 8, rh), F32),
            pltpu.VMEM((parts, n, rh, ffc), BF16),
            dma((semaphores(n, parts)[1],)),
        ],
        compiler_params=pltpu.CompilerParams(
            collective_id=0, has_side_effects=True, vmem_limit_bytes=60 * 2**20
        ),
    )(
        mix_gain[None, :], query_gain[None, :], mlp_gain[None, :],
        tokens, w_query, w_key, w_value, w_forget.T,
        key_cache.reshape(rows * gd, span),
        value_cache.reshape(rows * gd, span),
        decay_cache.reshape(rows * heads, span),
        w_out, w_up, w_down,
    )


def solution(mesh):
    in_specs = (
        P(None, "kv"),
        P("kv"),
        P("kv", "tp"),
        P("kv", "tp"),
        P("kv", "tp"),
        P("kv", "tp"),
        P(),
        P(None, "tp", None, "kv"),
        P(None, "tp", None, "kv"),
        P(None, "tp", "kv"),
        P("tp", "kv"),
        P("kv"),
        P("kv", "tp"),
        P("tp", "kv"),
    )
    body = functools.partial(shards, mesh.shape["kv"], mesh.shape["tp"])
    return jax.shard_map(
        body, mesh=mesh, in_specs=in_specs, out_specs=P(None, "kv"), check_vma=False
    )
```

```python
import functools

import jax
import jax.numpy as jnp
from jax import lax
from jax.experimental import pallas as pl
from jax.experimental.pallas import tpu as pltpu
from jax.sharding import PartitionSpec as P

MESH = pl.DeviceIdType.MESH
HEAD_DIM = 64
EPS = 1e-06
DEPTH = 256
PARTS = 2
F32 = jnp.float32
BF16 = jnp.bfloat16


def greet(n, t):
    kv, tp = lax.axis_index("kv"), lax.axis_index("tp")
    barrier = pltpu.get_barrier_semaphore()
    for i in range(1, n):
        pl.semaphore_signal(
            barrier, inc=1, device_id=(lax.rem(kv + i, n), tp), device_id_type=MESH
        )
    for i in range(1, t):
        pl.semaphore_signal(
            barrier, inc=1, device_id=(kv, lax.rem(tp + i, t)), device_id_type=MESH
        )
    pl.semaphore_wait(barrier, n + t - 2)


def flip(x, m):
    bit, y = 1, x
    while bit <= m:
        if m & bit:
            y = y + bit - 2 * bit * lax.rem(x // bit, 2)
        bit *= 2
    return y


def remote(src, dst, send, recv, kv, tp):
    return pltpu.make_async_remote_copy(
        src_ref=src,
        dst_ref=dst,
        send_sem=send,
        recv_sem=recv,
        device_id=(kv, tp),
        device_id_type=MESH,
    )


def semaphores(n, parts):
    half = n // 2
    sizes = dict(
        first=5, late=3, cache=3 * parts, q=2, e=2, x=2, g=2, m=1 + parts, a=1 + parts,
        t0=1 + parts, t1=1 + parts, y=1 + parts * half, s=1 + parts, z=1 + parts,
        along=1 + parts * half, across=1 + parts * half,
    )
    at, total = {}, 0
    for name, size in sizes.items():
        at[name] = total
        total += size
    return at, total


def split(x):
    hi = x.astype(BF16).astype(F32)
    return hi, (x - hi).astype(BF16).astype(F32)


def layer_kernel(
    n, t, d, sharing, parts,
    mgain, qgain, pgain, tok_hbm, wq_hbm, wk_hbm, wv_hbm, wf_hbm,
    k_hbm, v_hbm, d_hbm, wo_hbm, wu_hbm, wd_hbm, out,
    tok, wq, wk, wv, wf, kbuf, vbuf, dbuf, wo, wu, wd,
    stage_q, parts_s, got_s, partq, partx, gotq, gotx, qs, qall, own, msg, gotm, heads_s,
    att, allatt, full, tpa, tpb, upsend, upgot, upsend2, upgot2, keep, sqs, sqgot, hid,
    w_a, w_b, stat_a, stat_b, sem,
):
    kv, tp = lax.axis_index("kv"), lax.axis_index("tp")
    rows, dl = tok.shape
    rc = rows // n
    rh = rows // parts
    rb = rh // n
    nq, nk, heads = wq.shape[1], wk.shape[1], wf.shape[0]
    groups = heads // sharing
    gd = groups * HEAD_DIM
    lines = rb * heads
    pack = DEPTH // gd
    tile = pack * heads
    ffc = wu.shape[1] // n

    at_sem, _ = semaphores(n, parts)

    def flag(name, i=0):
        return sem.at[at_sem[name] + i]

    def local(src, dst, s):
        return pltpu.make_async_copy(src, dst, s)

    def drain(ref, s):
        pltpu.make_async_copy(ref, ref, s).wait()

    def block_of(i):
        return flip(kv, i)

    first = [
        local(a, b, flag("first", j))
        for j, (a, b) in enumerate(
            ((tok_hbm, tok), (wq_hbm, wq), (wk_hbm, wk), (wv_hbm, wv), (wf_hbm, wf))
        )
    ]
    for c in first:
        c.start()

    def cache_loads(h):
        at = pl.ds(h * rh * gd, rh * gd)
        lt = pl.ds(h * rh * heads, rh * heads)
        return (
            local(k_hbm.at[at], kbuf.at[at], flag("cache", 3 * h)),
            local(d_hbm.at[lt], dbuf.at[lt], flag("cache", 3 * h + 1)),
            local(v_hbm.at[at], vbuf.at[at], flag("cache", 3 * h + 2)),
        )

    for h in range(parts):
        for c in cache_loads(h):
            c.start()
    late = [
        local(a, b, flag("late", j))
        for j, (a, b) in enumerate(((wo_hbm, wo), (wu_hbm, wu), (wd_hbm, wd)))
    ]
    for c in late:
        c.start()
    greet(n, t)

    def send(name, src, dst, peer, slot=0):
        remote(src, dst, flag(name), flag(name, 1 + slot), peer, tp).start()

    def to_all(name, src, dst, slot=0):
        for i in range(n - 1, 0, -1):
            peer = block_of(i)
            send(name, src(peer), dst(i), peer, slot)

    for c in first:
        c.wait()
    stream = tok[...].astype(F32)
    squares = jnp.sum(stream * stream, axis=1, keepdims=True)
    normed = (stream * mgain[...]).astype(BF16)
    q = jnp.dot(normed, wq[...], preferred_element_type=F32)
    f = lax.dot_general(
        normed, wf[...], (((1,), (1,)), ((), ())), preferred_element_type=F32
    )
    pieces = [
        (p, slice(h * rb, (h + 1) * rb), slice(h * rh + p * rb, h * rh + (p + 1) * rb))
        for p in range(n)
        for h in range(parts)
    ]
    for p, to, cut in pieces:
        stage_q[p, to, :] = q[cut]
        parts_s[p, to, :] = jnp.broadcast_to(squares[cut], (rb, 128))
        parts_s[p, to, 0:heads] = f[cut]
    partq[...] = stage_q[...].astype(BF16)
    to_all("q", lambda p: partq.at[p], lambda i: gotq.at[i])
    to_all("e", lambda p: parts_s.at[p], lambda i: got_s.at[i])
    k = jnp.dot(normed, wk[...], preferred_element_type=F32)
    v = jnp.dot(normed, wv[...], preferred_element_type=F32)
    for p, to, cut in pieces:
        partx[p, to, 0:nk] = k[cut]
        partx[p, to, nk : 2 * nk] = v[cut]
    to_all("x", lambda p: partx.at[p], lambda i: gotx.at[i])

    total, stats = stage_q[kv], parts_s[kv]
    others = pl.ds(1, n - 1)
    drain(gotq.at[others], flag("q", 1))
    drain(got_s.at[others], flag("e", 1))
    for i in range(1, n):
        total = total + gotq[i].astype(F32)
        stats = stats + got_s[i]
    scale = lax.rsqrt(stats[:, 127:128] / d + EPS)
    raw = total * scale
    gate = stats[:, 0:heads] * scale
    forget = jnp.minimum(gate, 0.0) - jnp.log1p(jnp.exp(-jnp.abs(gate)))
    queries = []
    for h in range(heads):
        part = raw[:, h * HEAD_DIM : (h + 1) * HEAD_DIM]
        mean = jnp.sum(part * part, axis=1, keepdims=True) / HEAD_DIM
        part = (part * lax.rsqrt(mean + EPS) * qgain[...]).astype(BF16).astype(F32)
        queries.append(part)
    for j in range(sharing):
        side_by_side = [queries[g * sharing + j] for g in range(groups)]
        qs[pl.ds(j, rc, stride=sharing), :] = (
            jnp.concatenate(side_by_side, axis=1) if groups > 1 else side_by_side[0]
        )
    for h in range(parts):
        qall[kv, h] = qs[h * rb * sharing : (h + 1) * rb * sharing, :].astype(BF16)
    to_all("g", lambda p: qall.at[kv], lambda i: qall.at[kv])
    extra = partx[kv]
    drain(gotx.at[others], flag("x", 1))
    for i in range(1, n):
        extra = extra + gotx[i]
    extra = (extra * scale).astype(BF16).astype(F32)
    for h in range(heads):
        g = h // sharing
        key = extra[:, g * HEAD_DIM : (g + 1) * HEAD_DIM]
        value = extra[:, nk + g * HEAD_DIM : nk + (g + 1) * HEAD_DIM]
        score = jnp.sum(queries[h] * key, axis=1, keepdims=True) * (HEAD_DIM**-0.5)
        own[pl.ds(h, rc, stride=heads), :] = jnp.concatenate(
            [
                value,
                jnp.broadcast_to(score, (rc, 32)),
                jnp.broadcast_to(forget[:, h : h + 1], (rc, 32)),
            ],
            axis=1,
        )

    group_row = lax.broadcasted_iota(jnp.int32, (heads, gd), 0) // sharing
    group_lane = lax.broadcasted_iota(jnp.int32, (heads, gd), 1) // HEAD_DIM
    slot = lax.broadcasted_iota(jnp.int32, (HEAD_DIM, lines), 1) // sharing
    lane = lax.broadcasted_iota(jnp.int32, (tile, HEAD_DIM), 1) // 16

    steps = lines // tile
    many = max(1, 4 // steps) if parts > 1 else 2
    turns = n // many

    def blocks_at(u):
        at = (u % turns) * many
        return u // turns, [n - 1 - at - e for e in range(many)]

    def weigh(u, w_s, stat_s):
        h, peers = blocks_at(u)
        todo = [(block_of(i), s) for i in peers for s in range(steps)]
        scores = []
        for b, s in todo:
            qt = qall[b, h].astype(F32)
            strips = []
            for j in range(pack):
                at = (s * pack + j) * sharing
                one = jnp.concatenate([qt[at : at + sharing]] * groups, axis=0)
                one = jnp.where(group_row == group_lane, one, 0.0)
                zero = jnp.zeros_like(one)
                strips.append(
                    jnp.concatenate([one if m == j else zero for m in range(pack)], axis=1)
                )
            left = jnp.concatenate(strips, axis=0).astype(BF16)
            row = h * rh + b * rb + s * pack
            at = pl.ds(pl.multiple_of(row * gd, DEPTH), DEPTH)
            lt = pl.ds(pl.multiple_of(row * heads, tile), tile)
            scores.append(
                jnp.dot(left, kbuf[at, :], preferred_element_type=F32) * (HEAD_DIM**-0.5)
                + dbuf[lt, :]
            )
        for m, sc in enumerate(scores):
            hi, lo = split(jnp.max(sc, axis=1, keepdims=True))
            w = jnp.exp(sc - (hi + lo))
            mass = split(jnp.sum(w, axis=1, keepdims=True))
            w_s[m * tile : (m + 1) * tile, :] = w.astype(BF16)
            stat_s[m * tile : (m + 1) * tile, :] = jnp.where(
                lane == 0,
                hi,
                jnp.where(lane == 1, lo, jnp.where(lane == 2, mass[0], mass[1])),
            )

    def gather_values(u, w_s, stat_s):
        h, peers = blocks_at(u)
        for m, i in enumerate(peers):
            b = block_of(i)
            at = pl.ds(pl.multiple_of((h * rh + b * rb) * gd, rb * gd), rb * gd)
            mine = slice(m * lines, (m + 1) * lines)
            o = lax.dot_general(
                vbuf[at, :], w_s[mine, :], (((1,), (1,)), ((), ())),
                preferred_element_type=F32,
            )
            picked = o[0:HEAD_DIM]
            for g in range(1, rb * groups):
                picked = jnp.where(slot == g, o[g * HEAD_DIM : (g + 1) * HEAD_DIM], picked)
            msg[h, b] = jnp.concatenate([picked.T, stat_s[mine, :]], axis=1).astype(BF16)

    def message(u):
        h, peers = blocks_at(u)
        for i in peers:
            if i:
                b = block_of(i)
                send("m", msg.at[h, b], gotm.at[h, i], b, h)

    slots = (w_a, stat_a), (w_b, stat_b)

    def attend(u):
        if u + 1 < parts * turns:
            weigh(u + 1, *slots[(u + 1) % 2])
        gather_values(u, *slots[u % 2])
        message(u)

    def combine(h):
        extra = own[h * lines : (h + 1) * lines, :]
        own_score = extra[:, 64:65]
        forget = extra[:, 96:97]
        drain(gotm.at[h, others], flag("m", 1 + h))
        blocks = [msg[h, kv].astype(F32)] + [gotm[h, i].astype(F32) for i in range(1, n)]
        peaks = [b[:, 64:65] + b[:, 80:81] + forget for b in blocks]
        peak = own_score
        for p in peaks:
            peak = jnp.maximum(peak, p)
        own_weight = jnp.exp(own_score - peak)
        mass = own_weight
        summed = own_weight.astype(BF16).astype(F32) * extra[:, 0:64]
        for b, p in zip(blocks, peaks):
            w = jnp.exp(p - peak)
            mass = mass + w * (b[:, 96:97] + b[:, 112:113])
            summed = summed + w * b[:, 0:64]
        heads_s[h] = summed / mass
        for j in range(0, heads, 2):
            pair = [heads_s[h, pl.ds(j + m, rb, stride=heads), :] for m in range(2)]
            att[h, :, j * HEAD_DIM : (j + 2) * HEAD_DIM] = jnp.concatenate(
                pair, axis=1
            ).astype(BF16)
        allatt[h, kv] = att[h]
        to_all("a", lambda p: att.at[h], lambda i: allatt.at[h, kv], h)

    def tp_send(name, h, buf, value):
        buf[h, tp] = value.astype(BF16)
        for i in range(1, t):
            remote(
                buf.at[h, tp], buf.at[h, tp], flag(name), flag(name, 1 + h),
                kv, lax.rem(tp + i, t),
            ).start()

    def tp_total(name, h, buf):
        drain(buf.at[h, pl.ds(1, t - 1)], flag(name, 1 + h))
        total = buf[h, 0].astype(F32)
        for j in range(1, t):
            total = total + buf[h, j].astype(F32)
        return total.astype(BF16).astype(F32)

    def project_out(h):
        drain(allatt.at[h, others], flag("a", 1 + h))
        for p in range(n):
            full[h, p * rb : (p + 1) * rb, :] = allatt[h, p].astype(F32)
        attn = jnp.dot(full[h].astype(BF16), wo[...], preferred_element_type=F32)
        tp_send("t0", h, tpa, attn)

    half = n // 2
    side = lax.rem(kv, 2)
    place = kv // 2
    partner = kv + 1 - 2 * side
    order = list(range(half - 1, -1, -1))

    def across_z(j):
        return 2 * flip(place, j)

    def up_start(h):
        attn = tp_total("t0", h, tpa)
        residual = (tok[h * rh : (h + 1) * rh, :].astype(F32) + attn).astype(BF16).astype(F32)
        normed = (residual * pgain[...]).astype(BF16)

        def term(dest):
            cols = pl.ds(pl.multiple_of(dest * ffc, ffc), ffc)
            return jnp.dot(normed, wu[:, cols], preferred_element_type=F32)

        for j in order:
            upsend[h, j] = term(across_z(j) + 1 - side).astype(BF16)
            send("y", upsend.at[h, j], upgot.at[h, j], partner, h * half + j)
        for j in order:
            keep[h, j] = term(across_z(j) + side)
        sqs[h] = lax.dot_general(
            jnp.ones((8, dl), F32),
            residual * residual,
            (((1,), (1,)), ((), ())),
            preferred_element_type=F32,
            precision=lax.Precision.HIGHEST,
        )
        to_all("s", lambda p: sqs.at[h], lambda i: sqgot.at[h, i], h)
        return residual

    def up_middle(h):
        for j in order:
            drain(upgot.at[h, j], flag("y", 1 + h * half + j))
            part = keep[h, j] + upgot[h, j].astype(F32)
            if j:
                upsend2[h, j] = part.astype(BF16)
                send("z", upsend2.at[h, j], upgot2.at[h, j], across_z(j) + side, h)
        return part

    def up_finish(h, part):
        drain(sqgot.at[h, others], flag("s", 1 + h))
        total = sqs[h]
        for i in range(1, n):
            total = total + sqgot[h, i]
        r = lax.broadcasted_iota(jnp.int32, (rh, rh), 0)
        c_ = lax.broadcasted_iota(jnp.int32, (rh, rh), 1)
        wide = jnp.broadcast_to(total[0:1, :], (rh, rh))
        column = jnp.sum(jnp.where(r == c_, wide, 0.0), axis=1, keepdims=True)
        scale = lax.rsqrt(column / d + EPS)
        drain(upgot2.at[h, pl.ds(1, half - 1)], flag("z", 1 + h))
        for j in range(1, half):
            part = part + upgot2[h, j].astype(F32)
        hid[h, kv] = jnp.square(jnp.maximum(part * scale, 0.0)).astype(BF16)
        mine = hid.at[h, kv]
        send("across", mine, mine, partner, h * half)
        for j in order[:-1]:
            send("along", mine, mine, across_z(j) + side, h * half + j)

    def lower(h, src):
        there = pl.ds(pl.multiple_of(src * ffc, ffc), ffc)
        return jnp.dot(hid[h, src], wd[there, :], preferred_element_type=F32)

    def down_start(h):
        down = lower(h, kv)
        for j in order[:-1]:
            src = across_z(j) + side
            block = hid.at[h, src]
            drain(block, flag("along", 1 + h * half + j))
            send("across", block, block, partner, h * half + j)
            down = down + lower(h, src)
        return down

    def down_finish(h, down):
        for j in range(half):
            src = across_z(j) + 1 - side
            drain(hid.at[h, src], flag("across", 1 + h * half + j))
            down = down + lower(h, src)
        tp_send("t1", h, tpb, down)

    residuals, kept, downs = {}, {}, {}

    def stage_1(h):
        if h == 0:
            late[0].wait()
        project_out(h)

    def stage_2(h):
        if h == 0:
            late[1].wait()
        residuals[h] = up_start(h)

    def stage_3(h):
        kept[h] = up_middle(h)

    def stage_4(h):
        up_finish(h, kept[h])

    def stage_5(h):
        if h == 0:
            late[2].wait()
        downs[h] = down_start(h)

    def stage_6(h):
        down_finish(h, downs[h])

    def stage_7(h):
        out[h * rh : (h + 1) * rh, :] = (residuals[h] + tp_total("t1", h, tpb)).astype(BF16)

    stages = (combine, stage_1, stage_2, stage_3, stage_4, stage_5, stage_6, stage_7)
    share = 1.0 / parts
    gaps = (
        3.3, 4.5, 2.2 + 2.8 * share, 2.2 + 5.6 * share, 3.5, 3.6 + 2.8 * share,
        2.2 + 1.5 * share, 2.2 + 2.8 * share,
    )
    pace = 4.0 / (parts * turns)
    events = [(u * pace, 0, functools.partial(attend, u)) for u in range(parts * turns)]
    for h in range(parts):
        when = (h + 1) * turns * pace
        for stage, gap in zip(stages, gaps):
            when += gap
            events.append((when, 1 + h, functools.partial(stage, h)))
    events.sort(key=lambda e: e[:2])

    drain(qall.at[others], flag("g", 1))
    for h in range(parts):
        for c in cache_loads(h):
            c.wait()
    weigh(0, *slots[0])
    for _, _, event in events:
        event()
    rest = pl.ds(1, half - 1)
    drain(gotq.at[others], flag("q"))
    drain(got_s.at[others], flag("e"))
    drain(gotx.at[others], flag("x"))
    drain(qall.at[others], flag("g"))
    drain(gotm.at[:, others], flag("m"))
    drain(allatt.at[:, others], flag("a"))
    drain(tpa.at[:, pl.ds(1, t - 1)], flag("t0"))
    drain(upsend, flag("y"))
    drain(sqgot.at[:, others], flag("s"))
    drain(upgot2.at[:, rest], flag("z"))
    drain(upgot2.at[:, rest], flag("along"))
    drain(upgot, flag("across"))
    drain(tpb.at[:, pl.ds(1, t - 1)], flag("t1"))


def shards(
    n, t, tokens, mix_gain, w_query, w_key, w_value, w_forget, query_gain,
    key_cache, value_cache, decay_cache, w_out, mlp_gain, w_up, w_down,
):
    rows, dl = tokens.shape
    d = dl * n
    rc = rows // n
    heads = w_forget.shape[1]
    groups = key_cache.shape[1]
    sharing = heads // groups
    nq, nk = w_query.shape[1], w_key.shape[1]
    span = key_cache.shape[3]
    gd = groups * HEAD_DIM
    ffc = w_up.shape[1] // n
    half = n // 2
    pack = DEPTH // gd
    parts = PARTS if (rows // n) % (PARTS * pack) == 0 else 1
    rh = rows // parts
    rb = rh // n
    many = max(1, 4 // (rb // pack)) if parts > 1 else 2
    lines = rb * heads
    vmem = pl.BlockSpec(memory_space=pltpu.VMEM)
    anywhere = pl.BlockSpec(memory_space=pl.ANY)
    dma = pltpu.SemaphoreType.DMA
    return pl.pallas_call(
        functools.partial(layer_kernel, n, t, d, sharing, parts),
        out_shape=jax.ShapeDtypeStruct((rows, dl), BF16),
        in_specs=[vmem] * 3 + [anywhere] * 11,
        out_specs=vmem,
        scratch_shapes=[
            pltpu.VMEM(tokens.shape, BF16),
            pltpu.VMEM(w_query.shape, BF16),
            pltpu.VMEM(w_key.shape, BF16),
            pltpu.VMEM(w_value.shape, BF16),
            pltpu.VMEM((heads, dl), BF16),
            pltpu.VMEM((rows * gd, span), BF16),
            pltpu.VMEM((rows * gd, span), BF16),
            pltpu.VMEM((rows * heads, span), F32),
            pltpu.VMEM(w_out.shape, BF16),
            pltpu.VMEM(w_up.shape, BF16),
            pltpu.VMEM(w_down.shape, BF16),
            pltpu.VMEM((n, rc, nq), F32),
            pltpu.VMEM((n, rc, 128), F32),
            pltpu.VMEM((n, rc, 128), F32),
            pltpu.VMEM((n, rc, nq), BF16),
            pltpu.VMEM((n, rc, 2 * nk), F32),
            pltpu.VMEM((n, rc, nq), BF16),
            pltpu.VMEM((n, rc, 2 * nk), F32),
            pltpu.VMEM((rc * sharing, gd), F32),
            pltpu.VMEM((n, parts, rb * sharing, gd), BF16),
            pltpu.VMEM((rc * heads, 128), F32),
            pltpu.VMEM((parts, n, lines, 128), BF16),
            pltpu.VMEM((parts, n, lines, 128), BF16),
            pltpu.VMEM((parts, lines, HEAD_DIM), F32),
            pltpu.VMEM((parts, rb, nq), BF16),
            pltpu.VMEM((parts, n, rb, nq), BF16),
            pltpu.VMEM((parts, rh, nq), F32),
            pltpu.VMEM((parts, t, rh, dl), BF16),
            pltpu.VMEM((parts, t, rh, dl), BF16),
            pltpu.VMEM((parts, half, rh, ffc), BF16),
            pltpu.VMEM((parts, half, rh, ffc), BF16),
            pltpu.VMEM((parts, half, rh, ffc), BF16),
            pltpu.VMEM((parts, half, rh, ffc), BF16),
            pltpu.VMEM((parts, half, rh, ffc), F32),
            pltpu.VMEM((parts, 8, rh), F32),
            pltpu.VMEM((parts, n, 8, rh), F32),
            pltpu.VMEM((parts, n, rh, ffc), BF16),
            pltpu.VMEM((many * lines, span), BF16),
            pltpu.VMEM((many * lines, span), BF16),
            pltpu.VMEM((many * lines, HEAD_DIM), F32),
            pltpu.VMEM((many * lines, HEAD_DIM), F32),
            dma((semaphores(n, parts)[1],)),
        ],
        compiler_params=pltpu.CompilerParams(
            collective_id=0, has_side_effects=True, vmem_limit_bytes=60 * 2**20
        ),
    )(
        mix_gain[None, :], query_gain[None, :], mlp_gain[None, :],
        tokens, w_query, w_key, w_value, w_forget.T,
        key_cache.reshape(rows * gd, span),
        value_cache.reshape(rows * gd, span),
        decay_cache.reshape(rows * heads, span),
        w_out, w_up, w_down,
    )


def solution(mesh):
    in_specs = (
        P(None, "kv"),
        P("kv"),
        P("kv", "tp"),
        P("kv", "tp"),
        P("kv", "tp"),
        P("kv", "tp"),
        P(),
        P(None, "tp", None, "kv"),
        P(None, "tp", None, "kv"),
        P(None, "tp", "kv"),
        P("tp", "kv"),
        P("kv"),
        P("kv", "tp"),
        P("tp", "kv"),
    )
    body = functools.partial(shards, mesh.shape["kv"], mesh.shape["tp"])
    return jax.shard_map(
        body, mesh=mesh, in_specs=in_specs, out_specs=P(None, "kv"), check_vma=False
    )
```

```python
import functools

import jax
import jax.numpy as jnp
from jax import lax
from jax.experimental import pallas as pl
from jax.experimental.pallas import tpu as pltpu
from jax.sharding import PartitionSpec as P

MESH = pl.DeviceIdType.MESH
HEAD_DIM = 64
EPS = 1e-06
DEPTH = 256
PARTS = 2
F32 = jnp.float32
BF16 = jnp.bfloat16


def greet(n, t):
    kv, tp = lax.axis_index("kv"), lax.axis_index("tp")
    barrier = pltpu.get_barrier_semaphore()
    for i in range(1, n):
        pl.semaphore_signal(
            barrier, inc=1, device_id=(lax.rem(kv + i, n), tp), device_id_type=MESH
        )
    for i in range(1, t):
        pl.semaphore_signal(
            barrier, inc=1, device_id=(kv, lax.rem(tp + i, t)), device_id_type=MESH
        )
    pl.semaphore_wait(barrier, n + t - 2)


def flip(x, m):
    bit, y = 1, x
    while bit <= m:
        if m & bit:
            y = y + bit - 2 * bit * lax.rem(x // bit, 2)
        bit *= 2
    return y


def remote(src, dst, send, recv, kv, tp):
    return pltpu.make_async_remote_copy(
        src_ref=src,
        dst_ref=dst,
        send_sem=send,
        recv_sem=recv,
        device_id=(kv, tp),
        device_id_type=MESH,
    )


def semaphores(n, parts):
    half = n // 2
    sizes = dict(
        first=5, late=3, cache=3 * half, q=2, e=2, x=2, g=1 + n, m=1 + parts, a=1 + parts,
        t0=1 + parts, t1=1 + parts, y=1 + parts * half, s=1 + parts, z=1 + parts,
        along=1 + parts * half, across=1 + parts * half,
    )
    at, total = {}, 0
    for name, size in sizes.items():
        at[name] = total
        total += size
    return at, total


def split(x):
    hi = x.astype(BF16).astype(F32)
    return hi, (x - hi).astype(BF16).astype(F32)


def layer_kernel(
    n, t, d, sharing, parts,
    mgain, qgain, pgain, tok_hbm, wq_hbm, wk_hbm, wv_hbm, wf_hbm,
    k_hbm, v_hbm, d_hbm, wo_hbm, wu_hbm, wd_hbm, out,
    tok, wq, wk, wv, wf, kbuf, vbuf, dbuf, wo, wu, wd,
    stage_q, parts_s, got_s, partq, partx, gotq, gotx, qs, qall, own, msg, gotm, heads_s,
    att, allatt, full, tpa, tpb, upsend, upgot, upsend2, upgot2, keep, sqs, sqgot, hid,
    w_a, w_b, stat_a, stat_b, sem,
):
    kv, tp = lax.axis_index("kv"), lax.axis_index("tp")
    rows, dl = tok.shape
    rc = rows // n
    rh = rows // parts
    rb = rh // n
    nq, nk, heads = wq.shape[1], wk.shape[1], wf.shape[0]
    groups = heads // sharing
    gd = groups * HEAD_DIM
    lines = rb * heads
    pack = DEPTH // gd
    tile = pack * heads
    ffc = wu.shape[1] // n

    at_sem, _ = semaphores(n, parts)

    def flag(name, i=0):
        return sem.at[at_sem[name] + i]

    def local(src, dst, s):
        return pltpu.make_async_copy(src, dst, s)

    def drain(ref, s):
        pltpu.make_async_copy(ref, ref, s).wait()

    def block_of(i):
        return flip(kv, i)

    first = [
        local(a, b, flag("first", j))
        for j, (a, b) in enumerate(
            ((tok_hbm, tok), (wq_hbm, wq), (wk_hbm, wk), (wv_hbm, wv), (wf_hbm, wf))
        )
    ]
    for c in first:
        c.start()

    half = n // 2
    side = lax.rem(kv, 2)
    place = kv // 2
    partner = kv + 1 - 2 * side

    def cache_loads(j):
        z = flip(place, j)
        return [
            local(a.at[:, z], b.at[:, z], flag("cache", 3 * j + m))
            for m, (a, b) in enumerate(((k_hbm, kbuf), (d_hbm, dbuf), (v_hbm, vbuf)))
        ]

    near = [0, 1] + list(range(half - 1, 1, -1))
    for j in near:
        for c in cache_loads(j):
            c.start()
    late = [
        local(a, b, flag("late", j))
        for j, (a, b) in enumerate(((wo_hbm, wo), (wu_hbm, wu), (wd_hbm, wd)))
    ]
    for c in late:
        c.start()
    greet(n, t)

    def send(name, src, dst, peer, slot=0):
        remote(src, dst, flag(name), flag(name, 1 + slot), peer, tp).start()

    def to_all(name, src, dst, slot=0):
        for i in range(n - 1, 0, -1):
            peer = block_of(i)
            send(name, src(peer), dst(i), peer, slot)

    for c in first:
        c.wait()
    stream = tok[...].astype(F32)
    squares = jnp.sum(stream * stream, axis=1, keepdims=True)
    normed = (stream * mgain[...]).astype(BF16)
    q = jnp.dot(normed, wq[...], preferred_element_type=F32)
    f = lax.dot_general(
        normed, wf[...], (((1,), (1,)), ((), ())), preferred_element_type=F32
    )
    pieces = [
        (p, slice(h * rb, (h + 1) * rb), slice(h * rh + p * rb, h * rh + (p + 1) * rb))
        for p in range(n)
        for h in range(parts)
    ]
    for p, to, cut in pieces:
        stage_q[p, to, :] = q[cut]
        parts_s[p, to, :] = jnp.broadcast_to(squares[cut], (rb, 128))
        parts_s[p, to, 0:heads] = f[cut]
    partq[...] = stage_q[...].astype(BF16)
    to_all("q", lambda p: partq.at[p], lambda i: gotq.at[i])
    to_all("e", lambda p: parts_s.at[p], lambda i: got_s.at[i])
    k = jnp.dot(normed, wk[...], preferred_element_type=F32)
    v = jnp.dot(normed, wv[...], preferred_element_type=F32)
    for p, to, cut in pieces:
        partx[p, to, 0:nk] = k[cut]
        partx[p, to, nk : 2 * nk] = v[cut]
    to_all("x", lambda p: partx.at[p], lambda i: gotx.at[i])

    total, stats = stage_q[kv], parts_s[kv]
    others = pl.ds(1, n - 1)
    drain(gotq.at[others], flag("q", 1))
    drain(got_s.at[others], flag("e", 1))
    for i in range(1, n):
        total = total + gotq[i].astype(F32)
        stats = stats + got_s[i]
    scale = lax.rsqrt(stats[:, 127:128] / d + EPS)
    raw = total * scale
    gate = stats[:, 0:heads] * scale
    forget = jnp.minimum(gate, 0.0) - jnp.log1p(jnp.exp(-jnp.abs(gate)))
    queries = []
    for h in range(heads):
        part = raw[:, h * HEAD_DIM : (h + 1) * HEAD_DIM]
        mean = jnp.sum(part * part, axis=1, keepdims=True) / HEAD_DIM
        part = (part * lax.rsqrt(mean + EPS) * qgain[...]).astype(BF16).astype(F32)
        queries.append(part)
    for j in range(sharing):
        side_by_side = [queries[g * sharing + j] for g in range(groups)]
        qs[pl.ds(j, rc, stride=sharing), :] = (
            jnp.concatenate(side_by_side, axis=1) if groups > 1 else side_by_side[0]
        )
    for h in range(parts):
        qall[kv, h] = qs[h * rb * sharing : (h + 1) * rb * sharing, :].astype(BF16)
    for i in range(n - 1, 0, -1):
        send("g", qall.at[kv], qall.at[kv], block_of(i), i)
    group_row = lax.broadcasted_iota(jnp.int32, (heads, gd), 0) // sharing
    group_lane = lax.broadcasted_iota(jnp.int32, (heads, gd), 1) // HEAD_DIM
    slot = lax.broadcasted_iota(jnp.int32, (HEAD_DIM, lines), 1) // sharing
    lane = lax.broadcasted_iota(jnp.int32, (tile, HEAD_DIM), 1) // 16

    steps = lines // tile
    if parts == 2 and half > 2:
        far = [2 * j for j in near[2:]]
        ends = [[(m + 1, h), (m, h)] for h in range(2) for m in far]
        walk = [[(0, 0), (0, 1)], [(1, 0), (1, 1)]]
        walk += [[(3, 0), (2, 0)]] + ends[:len(far)] + ends[len(far):] + [[(3, 1), (2, 1)]]
    else:
        walk = [[(2 * j + 1, h), (2 * j, h)] for h in range(parts) for j in near]

    def weigh(u, w_s, stat_s):
        todo = [(i, h, s) for i, h in walk[u] for s in range(steps)]
        scores = []
        for i, h, s in todo:
            b = block_of(i)
            qt = qall[b, h].astype(F32)
            strips = []
            for j in range(pack):
                at = (s * pack + j) * sharing
                one = jnp.concatenate([qt[at : at + sharing]] * groups, axis=0)
                one = jnp.where(group_row == group_lane, one, 0.0)
                zero = jnp.zeros_like(one)
                strips.append(
                    jnp.concatenate([one if m == j else zero for m in range(pack)], axis=1)
                )
            left = jnp.concatenate(strips, axis=0).astype(BF16)
            low = lax.rem(b, 2)
            at = pl.ds(pl.multiple_of(low * rb * gd + s * DEPTH, DEPTH), DEPTH)
            lt = pl.ds(pl.multiple_of(low * lines + s * tile, tile), tile)
            scores.append(
                jnp.dot(left, kbuf[h, b // 2, at, :], preferred_element_type=F32)
                * (HEAD_DIM**-0.5)
                + dbuf[h, b // 2, lt, :]
            )
        for m, sc in enumerate(scores):
            hi, lo = split(jnp.max(sc, axis=1, keepdims=True))
            w = jnp.exp(sc - (hi + lo))
            mass = split(jnp.sum(w, axis=1, keepdims=True))
            w_s[m * tile : (m + 1) * tile, :] = w.astype(BF16)
            stat_s[m * tile : (m + 1) * tile, :] = jnp.where(
                lane == 0,
                hi,
                jnp.where(lane == 1, lo, jnp.where(lane == 2, mass[0], mass[1])),
            )

    def gather_values(u, w_s, stat_s):
        for m, (i, h) in enumerate(walk[u]):
            b = block_of(i)
            at = pl.ds(pl.multiple_of(lax.rem(b, 2) * rb * gd, rb * gd), rb * gd)
            mine = slice(m * lines, (m + 1) * lines)
            o = lax.dot_general(
                vbuf[h, b // 2, at, :], w_s[mine, :], (((1,), (1,)), ((), ())),
                preferred_element_type=F32,
            )
            picked = o[0:HEAD_DIM]
            for g in range(1, rb * groups):
                picked = jnp.where(slot == g, o[g * HEAD_DIM : (g + 1) * HEAD_DIM], picked)
            msg[h, b] = jnp.concatenate([picked.T, stat_s[mine, :]], axis=1).astype(BF16)

    def message(u):
        for i, h in walk[u]:
            if i:
                b = block_of(i)
                send("m", msg.at[h, b], gotm.at[h, i], b, h)

    slots = (w_a, stat_a), (w_b, stat_b)

    seen, loaded = set(), set()

    def ready(u):
        for i, h in walk[u]:
            if i and i not in seen:
                drain(qall.at[block_of(i)], flag("g", 1 + i))
            seen.add(i)
            if i // 2 not in loaded:
                for c in cache_loads(i // 2):
                    c.wait()
            loaded.add(i // 2)

    def attend(u):
        if u == 0:
            gather_values(u, *slots[0])
            own_terms()
        if u + 1 < len(walk):
            ready(u + 1)
            weigh(u + 1, *slots[(u + 1) % 2])
        if u:
            gather_values(u, *slots[u % 2])
        message(u)

    def own_terms():
        extra = partx[kv]
        drain(gotx.at[others], flag("x", 1))
        for i in range(1, n):
            extra = extra + gotx[i]
        extra = (extra * scale).astype(BF16).astype(F32)
        for h in range(heads):
            g = h // sharing
            key = extra[:, g * HEAD_DIM : (g + 1) * HEAD_DIM]
            value = extra[:, nk + g * HEAD_DIM : nk + (g + 1) * HEAD_DIM]
            score = jnp.sum(queries[h] * key, axis=1, keepdims=True) * (HEAD_DIM**-0.5)
            own[pl.ds(h, rc, stride=heads), :] = jnp.concatenate(
                [
                    value,
                    jnp.broadcast_to(score, (rc, 32)),
                    jnp.broadcast_to(forget[:, h : h + 1], (rc, 32)),
                ],
                axis=1,
            )

    def combine(h):
        extra = own[h * lines : (h + 1) * lines, :]
        own_score = extra[:, 64:65]
        forget = extra[:, 96:97]
        drain(gotm.at[h, others], flag("m", 1 + h))
        blocks = [msg[h, kv].astype(F32)] + [gotm[h, i].astype(F32) for i in range(1, n)]
        peaks = [b[:, 64:65] + b[:, 80:81] + forget for b in blocks]
        peak = own_score
        for p in peaks:
            peak = jnp.maximum(peak, p)
        own_weight = jnp.exp(own_score - peak)
        mass = own_weight
        summed = own_weight.astype(BF16).astype(F32) * extra[:, 0:64]
        for b, p in zip(blocks, peaks):
            w = jnp.exp(p - peak)
            mass = mass + w * (b[:, 96:97] + b[:, 112:113])
            summed = summed + w * b[:, 0:64]
        heads_s[h] = summed / mass
        for j in range(0, heads, 2):
            pair = [heads_s[h, pl.ds(j + m, rb, stride=heads), :] for m in range(2)]
            att[h, :, j * HEAD_DIM : (j + 2) * HEAD_DIM] = jnp.concatenate(
                pair, axis=1
            ).astype(BF16)
        allatt[h, kv] = att[h]
        to_all("a", lambda p: att.at[h], lambda i: allatt.at[h, kv], h)

    def tp_send(name, h, buf, value):
        buf[h, tp] = value.astype(BF16)
        for i in range(1, t):
            remote(
                buf.at[h, tp], buf.at[h, tp], flag(name), flag(name, 1 + h),
                kv, lax.rem(tp + i, t),
            ).start()

    def tp_total(name, h, buf):
        drain(buf.at[h, pl.ds(1, t - 1)], flag(name, 1 + h))
        total = buf[h, 0].astype(F32)
        for j in range(1, t):
            total = total + buf[h, j].astype(F32)
        return total.astype(BF16).astype(F32)

    def project_out(h):
        drain(allatt.at[h, others], flag("a", 1 + h))
        for p in range(n):
            full[h, p * rb : (p + 1) * rb, :] = allatt[h, p].astype(F32)
        attn = jnp.dot(full[h].astype(BF16), wo[...], preferred_element_type=F32)
        tp_send("t0", h, tpa, attn)

    order = list(range(half - 1, -1, -1))

    def across_z(j):
        return 2 * flip(place, j)

    def up_start(h):
        attn = tp_total("t0", h, tpa)
        residual = (tok[h * rh : (h + 1) * rh, :].astype(F32) + attn).astype(BF16).astype(F32)
        normed = (residual * pgain[...]).astype(BF16)

        def term(dest):
            cols = pl.ds(pl.multiple_of(dest * ffc, ffc), ffc)
            return jnp.dot(normed, wu[:, cols], preferred_element_type=F32)

        for j in order:
            upsend[h, j] = term(across_z(j) + 1 - side).astype(BF16)
            send("y", upsend.at[h, j], upgot.at[h, j], partner, h * half + j)
        for j in order:
            keep[h, j] = term(across_z(j) + side)
        sqs[h] = lax.dot_general(
            jnp.ones((8, dl), F32),
            residual * residual,
            (((1,), (1,)), ((), ())),
            preferred_element_type=F32,
            precision=lax.Precision.HIGHEST,
        )
        to_all("s", lambda p: sqs.at[h], lambda i: sqgot.at[h, i], h)
        return residual

    def up_middle(h):
        for j in order:
            drain(upgot.at[h, j], flag("y", 1 + h * half + j))
            part = keep[h, j] + upgot[h, j].astype(F32)
            if j:
                upsend2[h, j] = part.astype(BF16)
                send("z", upsend2.at[h, j], upgot2.at[h, j], across_z(j) + side, h)
        return part

    def up_finish(h, part):
        drain(sqgot.at[h, others], flag("s", 1 + h))
        total = sqs[h]
        for i in range(1, n):
            total = total + sqgot[h, i]
        r = lax.broadcasted_iota(jnp.int32, (rh, rh), 0)
        c_ = lax.broadcasted_iota(jnp.int32, (rh, rh), 1)
        wide = jnp.broadcast_to(total[0:1, :], (rh, rh))
        column = jnp.sum(jnp.where(r == c_, wide, 0.0), axis=1, keepdims=True)
        scale = lax.rsqrt(column / d + EPS)
        drain(upgot2.at[h, pl.ds(1, half - 1)], flag("z", 1 + h))
        for j in range(1, half):
            part = part + upgot2[h, j].astype(F32)
        hid[h, kv] = jnp.square(jnp.maximum(part * scale, 0.0)).astype(BF16)
        mine = hid.at[h, kv]
        send("across", mine, mine, partner, h * half)
        for j in order[:-1]:
            send("along", mine, mine, across_z(j) + side, h * half + j)

    def lower(h, src):
        there = pl.ds(pl.multiple_of(src * ffc, ffc), ffc)
        return jnp.dot(hid[h, src], wd[there, :], preferred_element_type=F32)

    def down_start(h):
        down = lower(h, kv)
        for j in order[:-1]:
            src = across_z(j) + side
            block = hid.at[h, src]
            drain(block, flag("along", 1 + h * half + j))
            send("across", block, block, partner, h * half + j)
            down = down + lower(h, src)
        return down

    def down_finish(h, down):
        for j in range(half):
            src = across_z(j) + 1 - side
            drain(hid.at[h, src], flag("across", 1 + h * half + j))
            down = down + lower(h, src)
        tp_send("t1", h, tpb, down)

    residuals, kept, downs = {}, {}, {}

    def stage_1(h):
        if h == 0:
            late[0].wait()
        project_out(h)

    def stage_2(h):
        if h == 0:
            late[1].wait()
        residuals[h] = up_start(h)

    def stage_3(h):
        kept[h] = up_middle(h)

    def stage_4(h):
        up_finish(h, kept[h])

    def stage_5(h):
        if h == 0:
            late[2].wait()
        downs[h] = down_start(h)

    def stage_6(h):
        down_finish(h, downs[h])

    def stage_7(h):
        out[h * rh : (h + 1) * rh, :] = (residuals[h] + tp_total("t1", h, tpb)).astype(BF16)

    stages = (combine, stage_1, stage_2, stage_3, stage_4, stage_5, stage_6, stage_7)
    ready(0)
    weigh(0, *slots[0])
    for u in range(len(walk)):
        attend(u)
    for stage in stages:
        for h in range(parts):
            stage(h)
    rest = pl.ds(1, half - 1)
    drain(gotq.at[others], flag("q"))
    drain(got_s.at[others], flag("e"))
    drain(gotx.at[others], flag("x"))
    drain(qall.at[others], flag("g"))
    drain(gotm.at[:, others], flag("m"))
    drain(allatt.at[:, others], flag("a"))
    drain(tpa.at[:, pl.ds(1, t - 1)], flag("t0"))
    drain(upsend, flag("y"))
    drain(sqgot.at[:, others], flag("s"))
    drain(upgot2.at[:, rest], flag("z"))
    drain(upgot2.at[:, rest], flag("along"))
    drain(upgot, flag("across"))
    drain(tpb.at[:, pl.ds(1, t - 1)], flag("t1"))


def shards(
    n, t, tokens, mix_gain, w_query, w_key, w_value, w_forget, query_gain,
    key_cache, value_cache, decay_cache, w_out, mlp_gain, w_up, w_down,
):
    rows, dl = tokens.shape
    d = dl * n
    rc = rows // n
    heads = w_forget.shape[1]
    groups = key_cache.shape[1]
    sharing = heads // groups
    nq, nk = w_query.shape[1], w_key.shape[1]
    span = key_cache.shape[3]
    gd = groups * HEAD_DIM
    ffc = w_up.shape[1] // n
    half = n // 2
    pack = DEPTH // gd
    parts = PARTS if (rows // n) % (PARTS * pack) == 0 else 1
    rh = rows // parts
    rb = rh // n
    lines = rb * heads
    vmem = pl.BlockSpec(memory_space=pltpu.VMEM)
    anywhere = pl.BlockSpec(memory_space=pl.ANY)
    dma = pltpu.SemaphoreType.DMA
    return pl.pallas_call(
        functools.partial(layer_kernel, n, t, d, sharing, parts),
        out_shape=jax.ShapeDtypeStruct((rows, dl), BF16),
        in_specs=[vmem] * 3 + [anywhere] * 11,
        out_specs=vmem,
        scratch_shapes=[
            pltpu.VMEM(tokens.shape, BF16),
            pltpu.VMEM(w_query.shape, BF16),
            pltpu.VMEM(w_key.shape, BF16),
            pltpu.VMEM(w_value.shape, BF16),
            pltpu.VMEM((heads, dl), BF16),
            pltpu.VMEM((parts, half, 2 * rb * gd, span), BF16),
            pltpu.VMEM((parts, half, 2 * rb * gd, span), BF16),
            pltpu.VMEM((parts, half, 2 * lines, span), F32),
            pltpu.VMEM(w_out.shape, BF16),
            pltpu.VMEM(w_up.shape, BF16),
            pltpu.VMEM(w_down.shape, BF16),
            pltpu.VMEM((n, rc, nq), F32),
            pltpu.VMEM((n, rc, 128), F32),
            pltpu.VMEM((n, rc, 128), F32),
            pltpu.VMEM((n, rc, nq), BF16),
            pltpu.VMEM((n, rc, 2 * nk), F32),
            pltpu.VMEM((n, rc, nq), BF16),
            pltpu.VMEM((n, rc, 2 * nk), F32),
            pltpu.VMEM((rc * sharing, gd), F32),
            pltpu.VMEM((n, parts, rb * sharing, gd), BF16),
            pltpu.VMEM((rc * heads, 128), F32),
            pltpu.VMEM((parts, n, lines, 128), BF16),
            pltpu.VMEM((parts, n, lines, 128), BF16),
            pltpu.VMEM((parts, lines, HEAD_DIM), F32),
            pltpu.VMEM((parts, rb, nq), BF16),
            pltpu.VMEM((parts, n, rb, nq), BF16),
            pltpu.VMEM((parts, rh, nq), F32),
            pltpu.VMEM((parts, t, rh, dl), BF16),
            pltpu.VMEM((parts, t, rh, dl), BF16),
            pltpu.VMEM((parts, half, rh, ffc), BF16),
            pltpu.VMEM((parts, half, rh, ffc), BF16),
            pltpu.VMEM((parts, half, rh, ffc), BF16),
            pltpu.VMEM((parts, half, rh, ffc), BF16),
            pltpu.VMEM((parts, half, rh, ffc), F32),
            pltpu.VMEM((parts, 8, rh), F32),
            pltpu.VMEM((parts, n, 8, rh), F32),
            pltpu.VMEM((parts, n, rh, ffc), BF16),
            pltpu.VMEM((2 * lines, span), BF16),
            pltpu.VMEM((2 * lines, span), BF16),
            pltpu.VMEM((2 * lines, HEAD_DIM), F32),
            pltpu.VMEM((2 * lines, HEAD_DIM), F32),
            dma((semaphores(n, parts)[1],)),
        ],
        compiler_params=pltpu.CompilerParams(
            collective_id=0, has_side_effects=True, vmem_limit_bytes=60 * 2**20
        ),
    )(
        mix_gain[None, :], query_gain[None, :], mlp_gain[None, :],
        tokens, w_query, w_key, w_value, w_forget.T,
        key_cache.reshape(parts, half, 2 * rb * gd, span),
        value_cache.reshape(parts, half, 2 * rb * gd, span),
        decay_cache.reshape(parts, half, 2 * lines, span),
        w_out, w_up, w_down,
    )


def solution(mesh):
    in_specs = (
        P(None, "kv"),
        P("kv"),
        P("kv", "tp"),
        P("kv", "tp"),
        P("kv", "tp"),
        P("kv", "tp"),
        P(),
        P(None, "tp", None, "kv"),
        P(None, "tp", None, "kv"),
        P(None, "tp", "kv"),
        P("tp", "kv"),
        P("kv"),
        P("kv", "tp"),
        P("tp", "kv"),
    )
    body = functools.partial(shards, mesh.shape["kv"], mesh.shape["tp"])
    return jax.shard_map(
        body, mesh=mesh, in_specs=in_specs, out_specs=P(None, "kv"), check_vma=False
    )
```
